128 devices in a mesh: sp: 16 (over z, y), tp: 8 (over x, core).
Axes of the slice: x: 4, y: 4, z: 4, core: 2. Of those that a mesh axis runs over, the one named last changes fastest.
Arguments:
- gate_branch: bfloat16 [12288, 1024], P('sp', 'tp'), may hold values from -6 to 6
- recur_input: bfloat16 [12288, 1024], P('sp', 'tp'), may hold values from -6 to 6
- doc_ids: int32 [12288], P('sp'), may hold values from 0 to 7, never falling along the last dimension, each value on 1 to 4608 neighbouring positions
- conv_taps: bfloat16 [4, 1024], P(None, 'tp'), may hold values from -3 to 3
- gate_map: bfloat16 [16, 64, 64], P('tp'), may hold values from -0.75 to 0.75
- input_map: bfloat16 [16, 64, 64], P('tp'), may hold values from -0.75 to 0.75
- decay_level: float32 [1024], P('tp'), may hold values from 4.8 to 12.3
- decay_extra: float32 [12288, 1024], P('sp', 'tp'), may hold values from -2.1 to -1.9e-05
- out_weight: bfloat16 [1024, 2048], P(None, 'tp'), may hold values from -0.7875 to 0.7875
- residual: bfloat16 [12288, 2048], P('sp', 'tp'), may hold values from -44 to 44
- mix_gain: float32 [2048], P('tp'), may hold values from 0.1 to 1.9
- pre_gain: float32 [2048], P('tp'), may hold values from 0.1 to 1.9
- ffn_gain: float32 [2048], P('tp'), may hold values from 0.1 to 1.9
- gate_weight: bfloat16 [2048, 5632], P('sp', 'tp'), may hold values from -0.125 to 0.125
- up_weight: bfloat16 [2048, 5632], P('sp', 'tp'), may hold values from -0.125 to 0.125
- down_weight: bfloat16 [5632, 2048], P('tp', 'sp'), may hold values from -0.33579113 to 0.33579113
Outputs:
- layer_out: bfloat16 [12288, 2048], P('sp', 'tp')
The draws below stay inside these ranges and needn't reach their ends.
Inputs may be any that keep to these rules, and one draw needn't show every extreme that they name: `doc_ids`: document numbers start at 0 and never fall along the sequence; a document has 1 to 4608 positions, and one has exactly that many.
All inputs are finite; a program needn't handle non-finite values.
Results may differ from the reference program's by a relative error of at most 0.013.
Values may be sent and summed in bfloat16 or wider, within the bound.
No kernel may reach another device: no remote copies, remote signals or barrier semaphores. Data moves between devices by JAX's collectives and lax.ppermute only.
A program may use at most 64 MiB of HBM per device.

```python
import math
import jax
import jax.numpy as jnp
import numpy as np
from jax import lax

D = 2048
W = 1024
HEAD = 64
FF = 5632
KCONV = 4
TOK_DEV = 768
TOKENS = 12288
DOCS = 8
N_TP = 8


def column_scales(key, columns, spread):
    ramp = jnp.exp(jnp.log(spread) * jnp.arange(columns, dtype=jnp.float32) / (columns - 1))
    jitter = jnp.exp(jax.random.uniform(key, (columns,), jnp.float32, math.log(0.7), math.log(1.4)))
    return ramp * jitter / math.sqrt(spread)


def scaled_matrix(key, row_count, columns):
    spread = 3.0
    keys = jax.random.split(key, 2)
    base = jnp.clip(jax.random.normal(keys[0], (row_count, columns), jnp.float32), -6.0, 6.0)
    return base * row_count ** (-0.5) * column_scales(keys[1], columns, spread)


def draw_out_weight(key, part):
    return scaled_matrix(jax.random.fold_in(key, 11), W, D).astype(jnp.bfloat16)


def draw_down_weight(key, part):
    return scaled_matrix(jax.random.fold_in(key, 12), FF, D).astype(jnp.bfloat16)


def draw_residual(key, part):
    keys = jax.random.split(jax.random.fold_in(key, 13), 3)
    spread = 3.0
    base = jnp.clip(jax.random.normal(keys[0], (TOKENS, D), jnp.float32), -6.0, 6.0)
    row_scale = jnp.exp(jax.random.uniform(keys[1], (TOKENS, 1), jnp.float32, math.log(0.3), math.log(3.0)))
    return (base * row_scale * column_scales(keys[2], D, spread)).astype(jnp.bfloat16)


def draw_decay_level(key, part):
    keys = jax.random.split(jax.random.fold_in(key, 14), 3)
    share = 0.5
    fast_heads = jax.random.uniform(keys[0], (W // HEAD, 1), jnp.float32) < share
    fast = jnp.broadcast_to(fast_heads, (W // HEAD, HEAD)).reshape(W)
    fast_rate = jnp.exp(jax.random.uniform(keys[1], (W,), jnp.float32, math.log(0.0025), math.log(0.008)))
    slow_rate = jnp.exp(jax.random.uniform(keys[2], (W,), jnp.float32, math.log(5e-06), math.log(2e-05)))
    target = jnp.where(fast, fast_rate, slow_rate)
    return -jnp.log(jnp.expm1(target))


def draw_decay_extra(key, part):
    keys = jax.random.split(jax.random.fold_in(key, 15), 3)
    blocks = TOKENS // TOK_DEV
    baseline = jnp.exp(jax.random.uniform(keys[0], (blocks, 1, W), jnp.float32, math.log(2e-05), math.log(0.0001)))
    baseline = jnp.broadcast_to(baseline, (blocks, TOK_DEV, W)).reshape(TOKENS, W)
    spots = jax.random.randint(keys[1], (3,), 0, TOKENS)
    hits = jnp.sum((jnp.arange(TOKENS)[:, None] == spots[None, :]).astype(jnp.float32), axis=1)
    kept = jax.random.uniform(keys[2], (TOKENS, W), jnp.float32, 0.5, 0.8)
    return -baseline + hits[:, None] * jnp.log(kept)


def level_of(stream_key, extent, cuts, low, high):
    def one(axis_at, blocks):
        draws = jax.random.uniform(jax.random.fold_in(jax.random.fold_in(stream_key, 6), axis_at), (blocks,), jnp.float32, low / len(cuts), high / len(cuts))
        return jnp.repeat(jnp.exp(draws), extent[axis_at] // blocks).reshape((-1,) + (1,) * (len(extent) - axis_at - 1))

    gain = one(*cuts[0])
    for cut in cuts[1:]:
        gain = gain * one(*cut)
    return gain


def length_profile(number_of, total, most, skew):
    loads = [(1 << 20) // math.isqrt(standing ** skew) + 1 for standing in range(2, number_of + 1)]
    spare, counts = total - most - (number_of - 1), [1] * (number_of - 1)
    while spare > 0:
        free = [i for i in range(number_of - 1) if counts[i] < most]
        whole, left = sum([loads[i] for i in free]), spare
        for i in free:
            addition = min(most - counts[i], max(1, left * loads[i] // whole), spare)
            counts[i] = counts[i] + addition
            spare = spare - addition
    return np.array([most] + counts)


def uneven_parts(stream_key, amount, total, most, lean):
    if amount == 2:
        one = jax.random.randint(stream_key, (), max(1, total - most), min(most, total - 1) + 1)
        return jnp.stack([one, total - one])
    sizes = jnp.asarray(length_profile(amount, total, most, lean), jnp.int32)
    couples = (amount - 1) // 2
    donor, taker = sizes[1:1 + 2 * couples:2], sizes[2:2 + 2 * couples:2]
    room = jnp.minimum(donor - 1, most - taker)
    passed = jax.random.randint(jax.random.fold_in(stream_key, 1), (couples,), 0, 1 << 20) % (room + 1)
    sizes = sizes.at[1:1 + 2 * couples:2].set(donor - passed).at[2:2 + 2 * couples:2].set(taker + passed)
    return sizes[jax.random.permutation(jax.random.fold_in(stream_key, 2), amount)]


def centred(key, shape, width, most, cuts=(), kind=jnp.bfloat16):
    loudness = level_of(key, shape, cuts, -0.22, 0.18) if cuts else 1.0
    entries = jax.random.normal(key, shape, jnp.float32) * width * loudness
    return jnp.minimum(jnp.maximum(entries, -most), most).astype(kind)


def setup_inputs(seed: int = 0) -> dict:
    arg_keys = jax.random.split(jax.random.key(seed), 17)
    return {
        "gate_branch": centred(arg_keys[0], (TOKENS, W), 1.0, 6.0, ((0, 16), (1, 8))),
        "recur_input": centred(arg_keys[1], (TOKENS, W), 1.0, 6.0, ((0, 16), (1, 8))),
        "doc_ids": jnp.searchsorted(jnp.cumsum(uneven_parts(arg_keys[2], DOCS, TOKENS, 6 * TOK_DEV, 0)), jnp.arange(TOKENS), side="right").astype(jnp.int32),
        "conv_taps": centred(arg_keys[3], (KCONV, W), 0.5, 3.0, ((1, 8),)),
        "gate_map": centred(arg_keys[4], (W // HEAD, HEAD, HEAD), HEAD ** -0.5, 0.75, ((0, 8),)),
        "input_map": centred(arg_keys[5], (W // HEAD, HEAD, HEAD), HEAD ** -0.5, 0.75, ((0, 8),)),
        "decay_level": draw_decay_level(jax.random.fold_in(arg_keys[16], 71), 0),
        "decay_extra": draw_decay_extra(jax.random.fold_in(arg_keys[16], 71), 0),
        "out_weight": draw_out_weight(jax.random.fold_in(arg_keys[16], 71), 0),
        "residual": draw_residual(jax.random.fold_in(arg_keys[16], 71), 0),
        "mix_gain": jnp.clip(1.0 + 0.18 * jax.random.normal(arg_keys[10], (D,), jnp.float32), 0.1, 1.9),
        "pre_gain": jnp.clip(1.0 + 0.18 * jax.random.normal(arg_keys[11], (D,), jnp.float32), 0.1, 1.9),
        "ffn_gain": jnp.clip(1.0 + 0.18 * jax.random.normal(arg_keys[12], (D,), jnp.float32), 0.1, 1.9),
        "gate_weight": centred(arg_keys[13], (D, FF), D ** -0.5, 0.125, ((0, 16), (1, 8))),
        "up_weight": centred(arg_keys[14], (D, FF), D ** -0.5, 0.125, ((0, 16), (1, 8))),
        "down_weight": draw_down_weight(jax.random.fold_in(arg_keys[16], 71), 0),
    }


epsilon = 1e-06
gate_power = 8.0

def combine(earlier, latter):
    return (earlier[0] * latter[0], latter[0] * earlier[1] + latter[1])

def inverse_rms(values, columns):
    return lax.rsqrt(lax.optimization_barrier(jnp.sum(values * values, axis=1, keepdims=True)) / columns + epsilon)

def reference(gate_branch, recur_input, doc_ids, conv_taps, gate_map, input_map, decay_level, decay_extra, out_weight, residual, mix_gain, pre_gain, ffn_gain, gate_weight, up_weight, down_weight):
    reach_rows = KCONV - 1
    padded_ids = jnp.concatenate([jnp.full((reach_rows,), -1, jnp.int32), doc_ids.astype(jnp.int32)])
    padded_rows = jnp.concatenate([jnp.zeros((reach_rows, W), jnp.float32), recur_input.astype(jnp.float32)])
    tap_weights = conv_taps.astype(jnp.float32)
    convolved = jnp.zeros((TOKENS, W), jnp.float32)
    for offset in range(KCONV):
        start_row = reach_rows - offset
        same_doc = (padded_ids[start_row:start_row + TOKENS] == doc_ids).astype(jnp.float32)[:, None]
        convolved = convolved + same_doc * padded_rows[start_row:start_row + TOKENS] * tap_weights[offset]
    conv_out = convolved.astype(jnp.bfloat16)
    head_rows = conv_out.astype(jnp.float32).reshape(TOKENS, W // HEAD, HEAD)
    recur_gate = jax.nn.sigmoid(jnp.einsum('thd,hde->the', head_rows, gate_map.astype(jnp.float32)).reshape(TOKENS, W))
    input_gate = jax.nn.sigmoid(jnp.einsum('thd,hde->the', head_rows, input_map.astype(jnp.float32)).reshape(TOKENS, W))
    log_decay = gate_power * -jax.nn.softplus(-decay_level) * recur_gate + decay_extra
    continues = (padded_ids[reach_rows - 1:reach_rows - 1 + TOKENS] == doc_ids).astype(jnp.float32)[:, None]
    factor = jnp.exp(log_decay) * continues
    driven = jnp.sqrt(-jnp.expm1(2.0 * log_decay)) * input_gate * conv_out.astype(jnp.float32)
    products, states = lax.associative_scan(combine, (factor, driven), axis=0)
    branch = (states * jax.nn.gelu(gate_branch.astype(jnp.float32))).astype(jnp.bfloat16)
    mixed_out = jnp.dot(branch, out_weight, preferred_element_type=jnp.float32).astype(jnp.bfloat16)
    mixed_f = mixed_out.astype(jnp.float32)
    stream = (residual.astype(jnp.float32) + mixed_f * inverse_rms(mixed_f, D) * mix_gain).astype(jnp.bfloat16)
    stream_f = stream.astype(jnp.float32)
    normed = (stream_f * inverse_rms(stream_f, D) * pre_gain).astype(jnp.bfloat16)
    gate_act = jnp.dot(normed, gate_weight, preferred_element_type=jnp.float32)
    up_act = jnp.dot(normed, up_weight, preferred_element_type=jnp.float32)
    hidden = (jax.nn.silu(gate_act) * up_act).astype(jnp.bfloat16)
    span_cols = FF // N_TP
    ffn_sum = jnp.zeros((TOKENS, D), jnp.float32)
    for member in range(N_TP):
        partial_value = jnp.dot(hidden[:, member * span_cols:(member + 1) * span_cols], down_weight[member * span_cols:(member + 1) * span_cols], preferred_element_type=jnp.float32)
        ffn_sum = ffn_sum + lax.optimization_barrier(partial_value.astype(jnp.bfloat16)).astype(jnp.float32)
    ffn_out = ffn_sum.astype(jnp.bfloat16)
    ffn_f = ffn_out.astype(jnp.float32)
    return (stream_f + ffn_f * inverse_rms(ffn_f, D) * ffn_gain).astype(jnp.bfloat16)
```

```python
import functools

import jax
import jax.numpy as jnp
from jax import lax
from jax.experimental import pallas as pl
from jax.experimental.pallas import tpu as pltpu
from jax.sharding import Mesh
from jax.sharding import PartitionSpec as P

SP = ("z", "y")
TP = ("x", "c")
EPS = 1e-06
BF = jnp.bfloat16
F32 = jnp.float32
VM = pl.BlockSpec(memory_space=pltpu.VMEM)
SM = pl.BlockSpec(memory_space=pltpu.SMEM)
HB = pl.BlockSpec(memory_space=pltpu.HBM)
SEGS = 8


def cyc(count, step):
    return [(i, (i + step) % count) for i in range(count)]


def stretch(row, lanes=128):
    return jnp.broadcast_to(row, (lanes, 128)).T


def taylor_expm1_neg(y):
    p = 1.0 + y * (1.0 / 8.0)
    for k in (7.0, 6.0, 5.0, 4.0, 3.0, 2.0):
        p = 1.0 + y * (1.0 / k) * p
    return -y * p


def pack_kernel(g_ref, u_ref, d_ref, out_ref):
    for j in range(5):
        at = slice(128 * j, 128 * j + 128)
        out_ref[at, :] = g_ref[:, at]
        out_ref[640 + 128 * j : 768 + 128 * j, :] = u_ref[:, at]
    out_ref[1280:1408, :] = jnp.concatenate([g_ref[:, 640:704], u_ref[:, 640:704]], axis=1)
    out_ref[1408:2112, :] = d_ref[...]


def scan_kernel(
    x_ref, rim_ref, ids_ref, taps_ref, gm_ref, im_ref, nsp_ref, extra_ref,
    s_ref, p_ref, e_ref, xs, idx, fs, ds,
):
    rows = x_ref.shape[0]
    taps = taps_ref[...].astype(F32)
    head = gm_ref.shape[1]

    def blockdiag(ref):
        zero = jnp.zeros((head, head), BF)
        return jnp.concatenate(
            [
                jnp.concatenate([ref[0], zero], axis=1),
                jnp.concatenate([zero, ref[1]], axis=1),
            ],
            axis=0,
        )

    gate = blockdiag(gm_ref)
    inp = blockdiag(im_ref)
    xs[0:8, :] = rim_ref[0:8, :]
    idx[0:8, :] = rim_ref[8:16, :]
    for j in range(rows // 128):
        at = 8 + 128 * j
        xs[at : at + 128, :] = x_ref[128 * j : 128 * j + 128, :].astype(F32)
        idx[at : at + 128, :] = stretch(ids_ref[j : j + 1, :])
    for j in range(rows // 128):
        at = 8 + 128 * j
        here = idx[at : at + 128, :]
        before = idx[at - 1 : at + 127, :]
        conv = xs[at : at + 128, :] * taps[0:1, :]
        for k in range(1, 4):
            old = idx[at - k : at - k + 128, :]
            conv = conv + jnp.where(old == here, xs[at - k : at - k + 128, :], 0.0) * taps[k : k + 1, :]
        conv = conv.astype(BF)
        rg = jax.nn.sigmoid(jnp.dot(conv, gate, preferred_element_type=F32))
        ig = jax.nn.sigmoid(jnp.dot(conv, inp, preferred_element_type=F32))
        ld = nsp_ref[...] * rg + extra_ref[128 * j : 128 * j + 128, :]
        e = jnp.exp(ld)
        y = 2.0 * ld
        em = jnp.where(y > -0.5, taylor_expm1_neg(jnp.maximum(y, -0.5)), 1.0 - e * e)
        fs[128 * j : 128 * j + 128, :] = jnp.where(before == here, e, 0.0)
        ds[128 * j : 128 * j + 128, :] = jnp.sqrt(em) * ig * conv.astype(F32)
    seg = rows // SEGS

    def step(j, carry):
        h, p = carry
        f = fs[pl.ds(j, SEGS, stride=seg), :]
        d = ds[pl.ds(j, SEGS, stride=seg), :]
        h = f * h + d
        p = p * f
        s_ref[pl.ds(j, SEGS, stride=seg), :] = h
        p_ref[pl.ds(j, SEGS, stride=seg), :] = p
        return h, p

    zero = jnp.zeros((SEGS, 128), F32)
    h, p = lax.fori_loop(0, seg, step, (zero, zero + 1.0), unroll=8)
    a = p[0:1, :]
    b = h[0:1, :]
    for s in range(1, SEGS):
        b = p[s : s + 1, :] * b + h[s : s + 1, :]
        a = p[s : s + 1, :] * a
    for i in range(16):
        e_ref[i, 0:1, :] = a
        e_ref[i, 1:2, :] = b


def branch_kernel(pos_ref, s_ref, p_ref, e_ref, g_ref, out_ref):
    rows = s_ref.shape[0]
    seg = rows // SEGS
    me = pos_ref[0]
    h = jnp.zeros((1, 128), F32)
    for i in range(16):
        a = e_ref[i, 0:1, :]
        b = e_ref[i, 1:2, :]
        h = jnp.where(i < me, a * h + b, h)
    half = SEGS // 2
    for s in range(SEGS):
        at = s * seg
        st = s_ref[at : at + seg, :]
        pr = p_ref[at : at + seg, :]
        states = st + pr * h
        out = (states * jax.nn.gelu(g_ref[at : at + seg, :].astype(F32), approximate=True)).astype(BF)
        h = states[seg - 1 : seg, :]
        to = (s % half) * seg
        for i in range(4):
            out_ref[2 * i + s // half, to : to + seg, :] = out


def mix_kernel(
    pos_ref, br_ref, w0, w1, w2, w3, v0, v1, v2, v3, g0, g1, g2, g3,
    norm_ref, keep_ref, send_ref, full, mixed, stream,
):
    x = pos_ref[2]
    c = pos_ref[1]
    rows = br_ref.shape[1]
    for i in range(8):
        full[:, 128 * i : 128 * i + 128] = br_ref[i]
    lhs = full[...]
    total = jnp.zeros((rows, 128), F32)
    pieces = []
    for d, w, v, g in ((0, w0, v0, g0), (3, w1, v1, g1), (1, w2, v2, g2), (2, w3, v3, g3)):
        block = lax.rem(x + d, 4)
        for k, core, ref in ((0, c, w), (1, 1 - c, v)):
            at = pl.ds(pl.multiple_of((2 * block + core) * 256, 256), 256)
            pieces.append((at, w, k, g))
            m = jnp.dot(lhs, ref[0:1024, :], preferred_element_type=F32).astype(BF)
            mixed[:, at] = m
            mf = m.astype(F32)
            mf = mf * mf
            total = total + mf[:, :128] + mf[:, 128:]
    scale = lax.rsqrt(jnp.sum(total, axis=1, keepdims=True) / 2048.0 + EPS)
    total = jnp.zeros((rows, 128), F32)
    for at, w, k, g in pieces:
        r = w[1024 + rows * k : 1024 + rows * k + rows, :].astype(F32)
        s = (r + mixed[:, at].astype(F32) * scale * g[2 * k : 2 * k + 1, :]).astype(BF)
        stream[:, at] = s
        sf = s.astype(F32)
        sf = sf * sf
        total = total + sf[:, :128] + sf[:, 128:]
    scale = lax.rsqrt(jnp.sum(total, axis=1, keepdims=True) / 2048.0 + EPS)
    for at, w, k, g in pieces:
        norm_ref[:, at] = (stream[:, at].astype(F32) * scale * g[2 * k + 1 : 2 * k + 2, :]).astype(BF)
    keep_ref[...] = stream[:, pl.ds(pl.multiple_of((2 * x + c) * 256, 256), 256)]
    send_ref[...] = stream[:, pl.ds(pl.multiple_of((2 * x + 1 - c) * 256, 256), 256)]


def down_copies(w_ref, dn, sem):
    return [
        pltpu.make_async_copy(w_ref.at[s, pl.ds(1408, 704)], dn.at[s], sem) for s in range(16)
    ]


def down_dot(lhs, dn, out_ref):
    for j in range(8):
        both = jnp.concatenate([dn[2 * j], dn[2 * j + 1]], axis=1)
        out_ref[:, 256 * j : 256 * j + 256] = jnp.dot(
            lhs, both, preferred_element_type=F32
        ).astype(BF)


def ffn_kernel(oth_ref, own_ref, w_ref, out_ref, hid_ref, gu, dn, hoth, sem):
    def tile(j):
        return [
            pltpu.make_async_copy(
                w_ref.at[s, pl.ds(128 * j, 128)], gu.at[j, pl.ds(128 * s, 128)], sem.at[j]
            )
            for s in range(16)
        ]

    order = [0, 5, 1, 6, 2, 7, 3, 8, 4, 9, 10]
    tiles = {j: tile(j) for j in order}
    downs = down_copies(w_ref, dn, sem.at[11])
    for j in order:
        for cp in tiles[j]:
            cp.start()
    for cp in downs:
        cp.start()
    for j in range(5):
        for k in (j, j + 5):
            for cp in tiles[k]:
                cp.wait()
        both = jnp.concatenate([gu[j], gu[j + 5]], axis=1)
        for src, dst in ((oth_ref, hoth), (own_ref, hid_ref)):
            act = jnp.dot(src[...], both, preferred_element_type=F32)
            dst[:, 128 * j : 128 * j + 128] = (jax.nn.silu(act[:, :128]) * act[:, 128:]).astype(BF)
    for cp in tiles[10]:
        cp.wait()
    for src, dst in ((oth_ref, hoth), (own_ref, hid_ref)):
        act = jnp.dot(src[...], gu[10], preferred_element_type=F32)
        dst[:, 640:704] = (jax.nn.silu(act[:, :64]) * act[:, 64:]).astype(BF)
    for cp in downs:
        cp.wait()
    down_dot(hoth[...], dn, out_ref)


def down_kernel(hid_ref, w_ref, out_ref, dn, sem):
    downs = down_copies(w_ref, dn, sem)
    for cp in downs:
        cp.start()
    for cp in downs:
        cp.wait()
    down_dot(hid_ref[...], dn, out_ref)


def summed(pos_ref, a_ref, b_ref, d, lo):
    h = a_ref.shape[0] // 2
    at = pl.ds(pl.multiple_of(lax.rem(pos_ref[2] + d, 4) * 512, 512), 512)
    return a_ref[lo : lo + h, at].astype(F32) + b_ref[lo : lo + h, at].astype(F32)


def far_kernel(pos_ref, a_ref, b_ref, right_ref, left_ref):
    h = a_ref.shape[0] // 2
    right_ref[...] = summed(pos_ref, a_ref, b_ref, 2, 0).astype(BF)
    left_ref[...] = summed(pos_ref, a_ref, b_ref, 2, h).astype(BF)


def near_kernel(pos_ref, a_ref, b_ref, right_ref, left_ref, accr_ref, accl_ref, own_ref):
    h = a_ref.shape[0] // 2
    right_ref[...] = summed(pos_ref, a_ref, b_ref, 1, h).astype(BF)
    left_ref[...] = summed(pos_ref, a_ref, b_ref, 3, 0).astype(BF)
    accr_ref[...] = summed(pos_ref, a_ref, b_ref, 1, 0)
    accl_ref[...] = summed(pos_ref, a_ref, b_ref, 3, h)
    own_ref[0:h, :] = summed(pos_ref, a_ref, b_ref, 0, 0)
    own_ref[h : 2 * h, :] = summed(pos_ref, a_ref, b_ref, 0, h)


def joined_kernel(pos_ref, own_ref, fl_ref, fr_ref, top_ref, bot_ref, keep_ref, send_ref, sq_ref):
    c = pos_ref[1]
    q = top_ref.shape[0]
    for k in range(2 * q // 64):
        lo = 64 * k
        at = slice(lo, lo + 64)
        if lo < q:
            more = fr_ref[at, :].astype(F32) + top_ref[at, :].astype(F32)
        else:
            more = fl_ref[lo - q : lo - q + 64, :].astype(F32) + bot_ref[lo - q : lo - q + 64, :].astype(F32)
        v = (own_ref[at, :] + more).astype(BF)
        for first, core in ((0, 0), (256, 1)):

            @pl.when(c == core)
            def _():
                keep_ref[at, :] = v[:, first : first + 256]

            @pl.when(c != core)
            def _():
                send_ref[at, :] = v[:, first : first + 256]

    for k in range(2 * q // 128):
        t = jnp.zeros((128, 128), F32)
        for ref in (keep_ref, send_ref):
            f = ref[128 * k : 128 * k + 128, :].astype(F32)
            f = f * f
            t = t + f[:, :128] + f[:, 128:]
        row = jnp.sum(t.T, axis=0, keepdims=True)
        for i in range(8):
            sq_ref[i, k : k + 1, :] = row


def final_kernel(pos_ref, keep_ref, got_ref, skeep_ref, sgot_ref, sq_ref, gain_ref, out_ref):
    c = pos_ref[1]
    half = keep_ref.shape[0]
    for f_ref, s_ref, core in ((keep_ref, skeep_ref, c), (got_ref, sgot_ref, 1 - c)):
        total = sq_ref[core]
        for i in range(1, 4):
            total = total + sq_ref[2 * i + core]
        scale = lax.rsqrt(total / 2048.0 + EPS)
        for k in range(half // 128):
            at = slice(128 * k, 128 * k + 128)
            col = stretch(scale[k : k + 1, :])
            for j in range(2):
                ln = slice(128 * j, 128 * j + 128)
                v = s_ref[at, ln].astype(F32) + f_ref[at, ln].astype(F32) * col * gain_ref[:, ln]
                out_ref[pl.ds(pl.multiple_of(core * half + 128 * k, 128), 128), ln] = v.astype(BF)


def call(fn, outs, specs, scratch=(), name=None):
    return pl.pallas_call(
        fn,
        out_shape=tuple(jax.ShapeDtypeStruct(s, d) for s, d in outs),
        in_specs=list(specs),
        out_specs=tuple(VM for _ in outs),
        scratch_shapes=list(scratch),
        name=name or fn.__name__,
    )


def swapped(block):
    return lax.ppermute(block, "c", cyc(2, 1))


def body(
    gate_branch, recur_input, doc_ids, conv_taps, gate_map, input_map, decay_level, decay_extra,
    out_weight, residual, mix_gain, pre_gain, ffn_gain, gate_weight, up_weight, down_weight,
):
    rows, width = recur_input.shape
    half = rows // 2
    x, c = lax.axis_index("x"), lax.axis_index("c")
    me = lax.axis_index(SP)
    pos = jnp.stack([me, c, x]).astype(jnp.int32)

    (stacked,) = call(pack_kernel, [((2112, 128), BF)], [VM] * 3)(
        gate_weight, up_weight, down_weight
    )
    weights = lax.all_gather(stacked, SP, axis=0)

    res_keep = lax.dynamic_slice_in_dim(residual, c * half, half, 0)
    res_send = lax.dynamic_slice_in_dim(residual, (1 - c) * half, half, 0)
    ahead = jnp.concatenate([out_weight, res_keep, swapped(res_send)])
    gains = jnp.stack([mix_gain, pre_gain])
    gains = jnp.concatenate([gains, swapped(gains)])
    near = [lax.ppermute(v, "x", cyc(4, d)) for v, d in ((ahead, 1), (ahead, 3), (gains, 1), (gains, 3), (gains, 2))]

    tail = jnp.pad(recur_input[rows - 3 :].astype(F32), ((5, 0), (0, 0)))
    tail_ids = jnp.pad(
        jnp.broadcast_to(doc_ids[rows - 3 :].astype(F32)[:, None], (3, width)), ((5, 0), (0, 0))
    )
    rim = lax.ppermute(
        jnp.concatenate([tail, tail_ids]), SP, [(i, i + 1) for i in range(15)]
    )
    nsp = (-8.0 * jax.nn.softplus(-decay_level))[None, :]
    states, products, ends = call(
        scan_kernel,
        [((rows, width), F32), ((rows, width), F32), ((16, 2, width), F32)],
        [VM] * 8,
        [
            pltpu.VMEM((rows + 8, width), F32),
            pltpu.VMEM((rows + 8, width), F32),
            pltpu.VMEM((rows, width), F32),
            pltpu.VMEM((rows, width), F32),
        ],
    )(
        recur_input, rim, doc_ids.astype(F32).reshape(rows // 128, 128), conv_taps, gate_map,
        input_map, nsp, decay_extra,
    )
    all_ends = lax.all_to_all(ends, SP, 0, 0, tiled=True)
    (branch,) = call(branch_kernel, [((8, half, width), BF)], [SM, VM, VM, VM, VM])(
        pos, states, products, all_ends, gate_branch
    )
    branch, near = lax.optimization_barrier((branch, near))
    branch = lax.all_to_all(branch, TP, 0, 0, tiled=True)
    from_left, from_right = near[:2]
    cut = from_left.shape[0] // 2
    far = jnp.concatenate(
        [
            lax.ppermute(from_left[:cut], "x", cyc(4, 1)),
            lax.ppermute(from_right[cut:], "x", cyc(4, 3)),
        ]
    )
    blocks = [ahead, from_left, from_right, far]
    norm_own, skeep, ssend = call(
        mix_kernel,
        [((half, 2048), BF), ((half, 256), BF), ((half, 256), BF)],
        [SM] + [VM] * 13,
        [
            pltpu.VMEM((half, 1024), BF),
            pltpu.VMEM((half, 2048), BF),
            pltpu.VMEM((half, 2048), BF),
        ],
    )(pos, branch, *blocks, *[swapped(b) for b in blocks], gains, *near[2:])
    norm_oth = swapped(norm_own)
    sgot = swapped(ssend)
    norm_own, norm_oth, skeep, sgot = lax.optimization_barrier((norm_own, norm_oth, skeep, sgot))

    part_oth, hid_own = call(
        ffn_kernel,
        [((half, 2048), BF), ((half, 704), BF)],
        [VM, VM, HB],
        [
            pltpu.VMEM((11, 2048, 128), BF),
            pltpu.VMEM((16, 704, 128), BF),
            pltpu.VMEM((half, 704), BF),
            pltpu.SemaphoreType.DMA((12,)),
        ],
    )(norm_oth, norm_own, weights)
    part_in = swapped(part_oth)
    (part_own,) = call(
        down_kernel,
        [((half, 2048), BF)],
        [VM, HB],
        [pltpu.VMEM((16, 704, 128), BF), pltpu.SemaphoreType.DMA],
    )(hid_own, weights)
    q = half // 2
    far_r, far_l = call(far_kernel, [((q, 512), BF)] * 2, [SM, VM, VM])(pos, part_own, part_in)
    near_r, near_l, acc_r, acc_l, own = call(
        near_kernel,
        [((q, 512), BF)] * 2 + [((q, 512), F32)] * 2 + [((half, 512), F32)],
        [SM, VM, VM],
    )(pos, part_own, part_in)
    pass_r = lax.ppermute(far_r, "x", cyc(4, 1))
    pass_l = lax.ppermute(far_l, "x", cyc(4, 3))
    from_left = lax.ppermute(near_r, "x", cyc(4, 1))
    from_right = lax.ppermute(near_l, "x", cyc(4, 3))
    pass_r, pass_l = lax.optimization_barrier((pass_r, pass_l))
    right2 = (pass_r.astype(F32) + acc_r).astype(BF)
    left2 = (pass_l.astype(F32) + acc_l).astype(BF)
    top = lax.ppermute(right2, "x", cyc(4, 1))
    bottom = lax.ppermute(left2, "x", cyc(4, 3))
    from_left, from_right, top, bottom = lax.optimization_barrier(
        (from_left, from_right, top, bottom)
    )
    fkeep, fsend, square = call(
        joined_kernel,
        [((half, 256), BF)] * 2 + [((8, 3, 128), F32)],
        [SM] + [VM] * 5,
    )(pos, own, from_left, from_right, top, bottom)
    fgot = swapped(fsend)
    square = lax.all_to_all(square, TP, 0, 0, tiled=True)
    (out,) = call(final_kernel, [((rows, 256), BF)], [SM] + [VM] * 6)(
        pos, fkeep, fgot, skeep, sgot, square, ffn_gain[None, :]
    )
    return out


def solution(mesh):
    split = Mesh(mesh.devices.reshape(4, 4, 4, 2), ("z", "y", "x", "c"))
    return jax.shard_map(
        body,
        mesh=split,
        in_specs=(
            P(SP, TP), P(SP, TP), P(SP), P(None, TP), P(TP, None, None), P(TP, None, None), P(TP),
            P(SP, TP), P(None, TP), P(SP, TP), P(TP), P(TP), P(TP), P(SP, TP), P(SP, TP), P(TP, SP),
        ),
        out_specs=P(SP, TP),
        check_vma=False,
    )
```

```python
import jax
import jax.numpy as jnp
from jax import lax
from jax.experimental import pallas as pl
from jax.experimental.pallas import tpu as pltpu
from jax.sharding import Mesh
from jax.sharding import PartitionSpec as P

SP = ("z", "y")
TP = ("x", "c")
EPS = 1e-06
BF = jnp.bfloat16
F32 = jnp.float32
VM = pl.BlockSpec(memory_space=pltpu.VMEM)
HB = pl.BlockSpec(memory_space=pltpu.HBM)
SEGS = 8


def cyc(count, step):
    return [(i, (i + step) % count) for i in range(count)]


def stretch(row, lanes=128):
    return jnp.broadcast_to(row, (lanes, 128)).T


def taylor_expm1_neg(y):
    p = 1.0 + y * (1.0 / 8.0)
    for k in (7.0, 6.0, 5.0, 4.0, 3.0, 2.0):
        p = 1.0 + y * (1.0 / k) * p
    return -y * p


def pack_kernel(g_ref, u_ref, d_ref, out_ref):
    for i, ref in enumerate((g_ref, u_ref, d_ref)):
        out_ref[704 * i : 704 * i + 704, :] = ref[...]


def scan_kernel(
    x_ref, rim_ref, ids_ref, taps_ref, gm_ref, im_ref, nsp_ref, extra_ref,
    s_ref, p_ref, e_ref, xs, idx, fs, ds,
):
    rows = x_ref.shape[0]
    taps = taps_ref[...].astype(F32)
    head = gm_ref.shape[1]

    def blockdiag(ref):
        zero = jnp.zeros((head, head), BF)
        return jnp.concatenate(
            [
                jnp.concatenate([ref[0], zero], axis=1),
                jnp.concatenate([zero, ref[1]], axis=1),
            ],
            axis=0,
        )

    gate = blockdiag(gm_ref)
    inp = blockdiag(im_ref)
    xs[0:8, :] = rim_ref[0:8, :]
    idx[0:8, :] = rim_ref[8:16, :]
    for j in range(rows // 128):
        at = 8 + 128 * j
        xs[at : at + 128, :] = x_ref[128 * j : 128 * j + 128, :].astype(F32)
        idx[at : at + 128, :] = stretch(ids_ref[j : j + 1, :])
    for j in range(rows // 128):
        at = 8 + 128 * j
        here = idx[at : at + 128, :]
        before = idx[at - 1 : at + 127, :]
        conv = xs[at : at + 128, :] * taps[0:1, :]
        for k in range(1, 4):
            old = idx[at - k : at - k + 128, :]
            conv = conv + jnp.where(old == here, xs[at - k : at - k + 128, :], 0.0) * taps[k : k + 1, :]
        conv = conv.astype(BF)
        rg = jax.nn.sigmoid(jnp.dot(conv, gate, preferred_element_type=F32))
        ig = jax.nn.sigmoid(jnp.dot(conv, inp, preferred_element_type=F32))
        ld = nsp_ref[...] * rg + extra_ref[128 * j : 128 * j + 128, :]
        e = jnp.exp(ld)
        y = 2.0 * ld
        em = jnp.where(y > -0.5, taylor_expm1_neg(jnp.maximum(y, -0.5)), 1.0 - e * e)
        fs[128 * j : 128 * j + 128, :] = jnp.where(before == here, e, 0.0)
        ds[128 * j : 128 * j + 128, :] = jnp.sqrt(em) * ig * conv.astype(F32)
    seg = rows // SEGS

    def step(j, carry):
        h, p = carry
        f = fs[pl.ds(j, SEGS, stride=seg), :]
        d = ds[pl.ds(j, SEGS, stride=seg), :]
        h = f * h + d
        p = p * f
        s_ref[pl.ds(j, SEGS, stride=seg), :] = h
        p_ref[pl.ds(j, SEGS, stride=seg), :] = p
        return h, p

    zero = jnp.zeros((SEGS, 128), F32)
    h, p = lax.fori_loop(0, seg, step, (zero, zero + 1.0), unroll=8)
    a = p[0:1, :]
    b = h[0:1, :]
    for s in range(1, SEGS):
        b = p[s : s + 1, :] * b + h[s : s + 1, :]
        a = p[s : s + 1, :] * a
    for i in range(16):
        e_ref[i, 0:1, :] = a
        e_ref[i, 1:2, :] = b


def branch_kernel(s_ref, p_ref, e_ref, g_ref, out_ref):
    rows = s_ref.shape[0]
    seg = rows // SEGS
    me = lax.axis_index(SP)
    h = jnp.zeros((1, 128), F32)
    for i in range(16):
        a = e_ref[i, 0:1, :]
        b = e_ref[i, 1:2, :]
        h = jnp.where(i < me, a * h + b, h)
    half = SEGS // 2
    for s in range(SEGS):
        at = s * seg
        st = s_ref[at : at + seg, :]
        pr = p_ref[at : at + seg, :]
        states = st + pr * h
        out = (states * jax.nn.gelu(g_ref[at : at + seg, :].astype(F32), approximate=True)).astype(BF)
        h = states[seg - 1 : seg, :]
        to = (s % half) * seg
        for i in range(4):
            out_ref[2 * i + s // half, to : to + seg, :] = out


def mix_kernel(
    br_ref, w0, w1, w2, w3, v0, v1, v2, v3, g_ref,
    norm_ref, keep_ref, send_ref, full, mixed, stream,
):
    x = lax.axis_index("x")
    c = lax.axis_index("c")
    rows = br_ref.shape[1]
    for i in range(8):
        full[:, 128 * i : 128 * i + 128] = br_ref[i]
    lhs = full[...]
    total = jnp.zeros((rows, 128), F32)
    pieces = []
    for d, w, v, g in ((0, w0, v0, 0), (3, w1, v1, 4), (1, w2, v2, 8), (2, w3, v3, 12)):
        block = lax.rem(x + d, 4)
        for k, core, ref in ((0, c, w), (1, 1 - c, v)):
            at = pl.ds(pl.multiple_of((2 * block + core) * 256, 256), 256)
            pieces.append((at, w, k, g))
            m = jnp.dot(lhs, ref[0:1024, :], preferred_element_type=F32).astype(BF)
            mixed[:, at] = m
            mf = m.astype(F32)
            mf = mf * mf
            total = total + mf[:, :128] + mf[:, 128:]
    scale = lax.rsqrt(jnp.sum(total, axis=1, keepdims=True) / 2048.0 + EPS)
    total = jnp.zeros((rows, 128), F32)
    for at, w, k, g in pieces:
        r = w[1024 + rows * k : 1024 + rows * k + rows, :].astype(F32)
        s = (r + mixed[:, at].astype(F32) * scale * g_ref[g + 2 * k : g + 2 * k + 1, :]).astype(BF)
        stream[:, at] = s
        sf = s.astype(F32)
        sf = sf * sf
        total = total + sf[:, :128] + sf[:, 128:]
    scale = lax.rsqrt(jnp.sum(total, axis=1, keepdims=True) / 2048.0 + EPS)
    for at, w, k, g in pieces:
        norm_ref[:, at] = (stream[:, at].astype(F32) * scale * g_ref[g + 2 * k + 1 : g + 2 * k + 2, :]).astype(BF)
    keep_ref[...] = stream[:, pl.ds(pl.multiple_of((2 * x + c) * 256, 256), 256)]
    send_ref[...] = stream[:, pl.ds(pl.multiple_of((2 * x + 1 - c) * 256, 256), 256)]


def down_copies(w_ref, dn, sem):
    return [
        pltpu.make_async_copy(w_ref.at[s, pl.ds(1408, 704)], dn.at[s], sem) for s in range(16)
    ]


def down_dot(lhs, dn, d):
    first = 4 * lax.rem(lax.axis_index("x") + d, 4)
    part = jnp.concatenate([dn[first + i] for i in range(4)], axis=1)
    return jnp.dot(lhs, part, preferred_element_type=F32).astype(BF)


def ffn_kernel(oth_ref, own_ref, w_ref, foth_ref, fown_ref, hoth, hid_ref, dn, gu, sem):
    cuts = ((0, 128), (128, 384), (384, 704))
    groups = []
    for i, (lo, hi) in enumerate(cuts):
        groups.append(
            [
                pltpu.make_async_copy(
                    w_ref.at[s, pl.ds(base + lo, hi - lo)],
                    gu.at[s, pl.ds(base + lo, hi - lo)],
                    sem.at[i],
                )
                for s in range(16)
                for base in (0, 704)
            ]
        )
    downs = down_copies(w_ref, dn, sem.at[3])
    for group in groups + [downs]:
        for cp in group:
            cp.start()
    turned = (((1,), (1,)), ((), ()))
    for (lo, hi), group in zip(cuts, groups):
        for cp in group:
            cp.wait()
        gate = jnp.concatenate([gu[s, lo:hi, :] for s in range(16)], axis=1)
        up = jnp.concatenate([gu[s, 704 + lo : 704 + hi, :] for s in range(16)], axis=1)
        for src, dst in ((oth_ref, hoth), (own_ref, hid_ref)):
            g = lax.dot_general(src[...], gate, turned, preferred_element_type=F32)
            u = lax.dot_general(src[...], up, turned, preferred_element_type=F32)
            dst[:, lo:hi] = (jax.nn.silu(g) * u).astype(BF)
    for cp in downs:
        cp.wait()
    foth_ref[...] = down_dot(hoth[...], dn, 2)
    fown_ref[...] = down_dot(hid_ref[...], dn, 2)


def down_kernel(hoth_ref, hid_ref, dn, oth_ref, own_ref):
    for src, dst in ((hoth_ref, oth_ref), (hid_ref, own_ref)):
        lhs = src[...]
        for i, d in enumerate((1, 3, 0)):
            dst[i] = down_dot(lhs, dn, d)


def far_kernel(a_ref, b_ref, right_ref, left_ref):
    h = a_ref.shape[0] // 2
    total = a_ref[...].astype(F32) + b_ref[...].astype(F32)
    right_ref[...] = total[:h].astype(BF)
    left_ref[...] = total[h:].astype(BF)


def near_kernel(a_ref, b_ref, right_ref, left_ref, accr_ref, accl_ref, own_ref):
    h = a_ref.shape[1] // 2
    right_ref[...] = (a_ref[0, h:].astype(F32) + b_ref[0, h:].astype(F32)).astype(BF)
    left_ref[...] = (a_ref[1, :h].astype(F32) + b_ref[1, :h].astype(F32)).astype(BF)
    accr_ref[...] = a_ref[0, :h].astype(F32) + b_ref[0, :h].astype(F32)
    accl_ref[...] = a_ref[1, h:].astype(F32) + b_ref[1, h:].astype(F32)
    own_ref[...] = a_ref[2].astype(F32) + b_ref[2].astype(F32)


def relay_kernel(r_ref, l_ref, accr_ref, accl_ref, right_ref, left_ref):
    right_ref[...] = (r_ref[...].astype(F32) + accr_ref[...]).astype(BF)
    left_ref[...] = (l_ref[...].astype(F32) + accl_ref[...]).astype(BF)


def joined_kernel(own_ref, fl_ref, fr_ref, top_ref, bot_ref, keep_ref, send_ref, sq_ref):
    c = lax.axis_index("c")
    q = top_ref.shape[0]
    for k in range(2 * q // 64):
        lo = 64 * k
        at = slice(lo, lo + 64)
        if lo < q:
            more = fr_ref[at, :].astype(F32) + top_ref[at, :].astype(F32)
        else:
            more = fl_ref[lo - q : lo - q + 64, :].astype(F32) + bot_ref[lo - q : lo - q + 64, :].astype(F32)
        v = (own_ref[at, :] + more).astype(BF)
        for first, core in ((0, 0), (256, 1)):

            @pl.when(c == core)
            def _():
                keep_ref[at, :] = v[:, first : first + 256]

            @pl.when(c != core)
            def _():
                send_ref[at, :] = v[:, first : first + 256]

    for k in range(2 * q // 128):
        t = jnp.zeros((128, 128), F32)
        for ref in (keep_ref, send_ref):
            f = ref[128 * k : 128 * k + 128, :].astype(F32)
            f = f * f
            t = t + f[:, :128] + f[:, 128:]
        row = jnp.sum(t.T, axis=0, keepdims=True)
        for i in range(8):
            sq_ref[i, k : k + 1, :] = row


def final_kernel(keep_ref, got_ref, skeep_ref, sgot_ref, sq_ref, gain_ref, out_ref):
    c = lax.axis_index("c")
    half = keep_ref.shape[0]
    for f_ref, s_ref, core in ((keep_ref, skeep_ref, c), (got_ref, sgot_ref, 1 - c)):
        total = sq_ref[core]
        for i in range(1, 4):
            total = total + sq_ref[2 * i + core]
        scale = lax.rsqrt(total / 2048.0 + EPS)
        for k in range(half // 128):
            at = slice(128 * k, 128 * k + 128)
            col = stretch(scale[k : k + 1, :])
            for j in range(2):
                ln = slice(128 * j, 128 * j + 128)
                v = s_ref[at, ln].astype(F32) + f_ref[at, ln].astype(F32) * col * gain_ref[:, ln]
                out_ref[pl.ds(pl.multiple_of(core * half + 128 * k, 128), 128), ln] = v.astype(BF)


def call(fn, outs, specs, scratch=(), limit=8):
    return pl.pallas_call(
        fn,
        out_shape=tuple(jax.ShapeDtypeStruct(s, d) for s, d in outs),
        in_specs=list(specs),
        out_specs=tuple(VM for _ in outs),
        scratch_shapes=list(scratch),
        compiler_params=pltpu.CompilerParams(vmem_limit_bytes=limit << 20),
    )


def kept_in_hbm(*arrays):
    return [pltpu.with_memory_space_constraint(a, pltpu.HBM) for a in arrays]


def swapped(block):
    return lax.ppermute(block, "c", cyc(2, 1))


def steps(
    gate_branch, recur_input, doc_ids, conv_taps, gate_map, input_map, decay_level, decay_extra,
    out_weight, residual, mix_gain, pre_gain, ffn_gain, gate_weight, up_weight, down_weight,
):
    rows, width = recur_input.shape
    half = rows // 2
    c = lax.axis_index("c")

    (stacked,) = call(
        pack_kernel, [((2112, 128), BF)], [VM] * 3
    )(*kept_in_hbm(gate_weight.T, up_weight.T, down_weight))
    (weights,) = kept_in_hbm(lax.all_gather(stacked, SP, axis=0))

    res_keep = lax.dynamic_slice_in_dim(residual, c * half, half, 0)
    res_send = lax.dynamic_slice_in_dim(residual, (1 - c) * half, half, 0)
    ahead = jnp.concatenate([out_weight, res_keep, swapped(res_send)])
    from_left = lax.ppermute(ahead, "x", cyc(4, 1))
    from_right = lax.ppermute(ahead, "x", cyc(4, 3))
    gains = jnp.stack([mix_gain, pre_gain])
    gains = jnp.concatenate([gains, swapped(gains)])
    all_gains = [gains]
    for d in (1, 3, 2):
        all_gains.append(lax.ppermute(gains, "x", cyc(4, d)))

    tail = jnp.pad(recur_input[rows - 3 :].astype(F32), ((5, 0), (0, 0)))
    tail_ids = jnp.pad(
        jnp.broadcast_to(doc_ids[rows - 3 :].astype(F32)[:, None], (3, width)), ((5, 0), (0, 0))
    )
    rim = lax.ppermute(
        jnp.concatenate([tail, tail_ids]), SP, [(i, i + 1) for i in range(15)]
    )
    nsp = (-8.0 * jax.nn.softplus(-decay_level))[None, :]
    states, products, ends = call(
        scan_kernel,
        [((rows, width), F32), ((rows, width), F32), ((16, 2, width), F32)],
        [VM] * 8,
        [
            pltpu.VMEM((rows + 8, width), F32),
            pltpu.VMEM((rows + 8, width), F32),
            pltpu.VMEM((rows, width), F32),
            pltpu.VMEM((rows, width), F32),
        ],
    )(
        *kept_in_hbm(recur_input),
        rim,
        doc_ids.astype(F32).reshape(rows // 128, 128),
        *kept_in_hbm(conv_taps, gate_map, input_map),
        nsp,
        *kept_in_hbm(decay_extra),
    )
    all_ends = lax.all_to_all(ends, SP, 0, 0, tiled=True)
    (branch,) = call(branch_kernel, [((8, half, width), BF)], [VM] * 4)(
        states, products, all_ends, *kept_in_hbm(gate_branch)
    )
    branch = lax.all_to_all(branch, TP, 0, 0, tiled=True)
    cut = from_left.shape[0] // 2
    far_top = lax.ppermute(from_left[:cut], "x", cyc(4, 1))
    far_bottom = lax.ppermute(from_right[cut:], "x", cyc(4, 3))
    far = jnp.concatenate([far_top, far_bottom])
    blocks = [ahead, from_left, from_right, far]
    others = [swapped(b) for b in blocks[:3]]
    others.append(swapped(far))
    norm_own, skeep, ssend = call(
        mix_kernel,
        [((half, 2048), BF), ((half, 256), BF), ((half, 256), BF)],
        [VM] * 10,
        [
            pltpu.VMEM((half, 1024), BF),
            pltpu.VMEM((half, 2048), BF),
            pltpu.VMEM((half, 2048), BF),
        ],
        limit=12,
    )(branch, *blocks, *others, jnp.concatenate(all_gains))
    norm_oth = swapped(norm_own)
    sgot = swapped(ssend)

    far_oth, far_own, hid_oth, hid_own, down = call(
        ffn_kernel,
        [((half, 512), BF)] * 2 + [((half, 704), BF)] * 2 + [((16, 704, 128), BF)],
        [VM, VM, HB],
        [pltpu.VMEM((16, 1408, 128), BF), pltpu.SemaphoreType.DMA((4,))],
        limit=15,
    )(norm_oth, norm_own, weights)
    far_in = swapped(far_oth)
    rest_oth, rest_own = call(
        down_kernel, [((3, half, 512), BF)] * 2, [VM] * 3, limit=14
    )(hid_oth, hid_own, down)
    rest_in = swapped(rest_oth)
    q = half // 2
    far_r, far_l = call(far_kernel, [((q, 512), BF)] * 2, [VM] * 2)(far_own, far_in)
    pass_r = lax.ppermute(far_r, "x", cyc(4, 1))
    pass_l = lax.ppermute(far_l, "x", cyc(4, 3))
    near_r, near_l, acc_r, acc_l, own = call(
        near_kernel,
        [((q, 512), BF)] * 2 + [((q, 512), F32)] * 2 + [((half, 512), F32)],
        [VM] * 2,
        limit=10,
    )(rest_own, rest_in)
    from_left = lax.ppermute(near_r, "x", cyc(4, 1))
    from_right = lax.ppermute(near_l, "x", cyc(4, 3))
    pass_r, pass_l = lax.optimization_barrier((pass_r, pass_l))
    right2, left2 = call(relay_kernel, [((q, 512), BF)] * 2, [VM] * 4)(pass_r, pass_l, acc_r, acc_l)
    top = lax.ppermute(right2, "x", cyc(4, 1))
    bottom = lax.ppermute(left2, "x", cyc(4, 3))
    from_left, from_right, top, bottom = lax.optimization_barrier(
        (from_left, from_right, top, bottom)
    )
    fkeep, fsend, square = call(
        joined_kernel,
        [((half, 256), BF)] * 2 + [((8, 3, 128), F32)],
        [VM] * 5,
    )(own, from_left, from_right, top, bottom)
    fgot = swapped(fsend)
    square = lax.all_to_all(square, TP, 0, 0, tiled=True)
    (out,) = call(final_kernel, [((rows, 256), BF)], [VM] * 6)(
        fkeep, fgot, skeep, sgot, square, ffn_gain[None, :]
    )
    return out


def solution(mesh):
    split = Mesh(mesh.devices.reshape(4, 4, 4, 2), ("z", "y", "x", "c"))
    return jax.shard_map(
        steps,
        mesh=split,
        in_specs=(
            P(SP, TP), P(SP, TP), P(SP), P(None, TP), P(TP, None, None), P(TP, None, None), P(TP),
            P(SP, TP), P(None, TP), P(SP, TP), P(TP), P(TP), P(TP), P(SP, TP), P(SP, TP), P(TP, SP),
        ),
        out_specs=P(SP, TP),
        check_vma=False,
    )
```

```python
import jax
import jax.numpy as jnp
from jax import lax
from jax.experimental import pallas as pl
from jax.experimental.pallas import tpu as pltpu
from jax.sharding import Mesh
from jax.sharding import PartitionSpec as P

SP = ("z", "y")
TP = ("x", "c")
EPS = 1e-06
BF = jnp.bfloat16
F32 = jnp.float32
VM = pl.BlockSpec(memory_space=pltpu.VMEM)
HB = pl.BlockSpec(memory_space=pltpu.HBM)
SEGS = 8


def cyc(count, step):
    return [(i, (i + step) % count) for i in range(count)]


def stretch(row, lanes=128):
    return jnp.broadcast_to(row, (lanes, 128)).T


def taylor_expm1_neg(y):
    p = 1.0 + y * (1.0 / 8.0)
    for k in (7.0, 6.0, 5.0, 4.0, 3.0, 2.0):
        p = 1.0 + y * (1.0 / k) * p
    return -y * p


def pack_kernel(g_ref, u_ref, d_ref, out_ref, buf, sem):
    spans = [pl.ds(704 * i, 704) for i in range(3)]
    fetches = [
        pltpu.make_async_copy(ref, buf.at[span], sem.at[i])
        for i, (ref, span) in enumerate(zip((g_ref, u_ref, d_ref), spans))
    ]
    stores = [
        pltpu.make_async_copy(buf.at[span], out_ref.at[span], sem.at[3 + i])
        for i, span in enumerate(spans)
    ]
    for cp in fetches:
        cp.start()
    for cp, then in zip(fetches, stores):
        cp.wait()
        then.start()
    for cp in stores:
        cp.wait()


def scan_kernel(
    x_ref, rim_ref, ids_ref, taps_ref, gm_ref, im_ref, nsp_ref, extra_ref,
    s_ref, p_ref, e_ref, xs, idx, fs, ds,
):
    rows = x_ref.shape[0]
    taps = taps_ref[...].astype(F32)
    head = gm_ref.shape[1]

    def blockdiag(ref):
        zero = jnp.zeros((head, head), BF)
        return jnp.concatenate(
            [
                jnp.concatenate([ref[0], zero], axis=1),
                jnp.concatenate([zero, ref[1]], axis=1),
            ],
            axis=0,
        )

    gate = blockdiag(gm_ref)
    inp = blockdiag(im_ref)
    xs[0:8, :] = rim_ref[0:8, :]
    idx[0:8, :] = rim_ref[8:16, :]
    for j in range(rows // 128):
        at = 8 + 128 * j
        xs[at : at + 128, :] = x_ref[128 * j : 128 * j + 128, :].astype(F32)
        idx[at : at + 128, :] = stretch(ids_ref[j : j + 1, :])
    for j in range(rows // 128):
        at = 8 + 128 * j
        here = idx[at : at + 128, :]
        before = idx[at - 1 : at + 127, :]
        conv = xs[at : at + 128, :] * taps[0:1, :]
        for k in range(1, 4):
            old = idx[at - k : at - k + 128, :]
            conv = conv + jnp.where(old == here, xs[at - k : at - k + 128, :], 0.0) * taps[k : k + 1, :]
        conv = conv.astype(BF)
        rg = jax.nn.sigmoid(jnp.dot(conv, gate, preferred_element_type=F32))
        ig = jax.nn.sigmoid(jnp.dot(conv, inp, preferred_element_type=F32))
        ld = nsp_ref[...] * rg + extra_ref[128 * j : 128 * j + 128, :]
        e = jnp.exp(ld)
        y = 2.0 * ld
        em = jnp.where(y > -0.5, taylor_expm1_neg(jnp.maximum(y, -0.5)), 1.0 - e * e)
        fs[128 * j : 128 * j + 128, :] = jnp.where(before == here, e, 0.0)
        ds[128 * j : 128 * j + 128, :] = jnp.sqrt(em) * ig * conv.astype(F32)
    seg = rows // SEGS

    def step(j, carry):
        h, p = carry
        f = fs[pl.ds(j, SEGS, stride=seg), :]
        d = ds[pl.ds(j, SEGS, stride=seg), :]
        h = f * h + d
        p = p * f
        s_ref[pl.ds(j, SEGS, stride=seg), :] = h
        p_ref[pl.ds(j, SEGS, stride=seg), :] = p
        return h, p

    zero = jnp.zeros((SEGS, 128), F32)
    h, p = lax.fori_loop(0, seg, step, (zero, zero + 1.0), unroll=8)
    a = p[0:1, :]
    b = h[0:1, :]
    for s in range(1, SEGS):
        b = p[s : s + 1, :] * b + h[s : s + 1, :]
        a = p[s : s + 1, :] * a
    for i in range(16):
        e_ref[i, 0:1, :] = a
        e_ref[i, 1:2, :] = b


def branch_kernel(s_ref, p_ref, e_ref, g_ref, out_ref):
    rows = s_ref.shape[0]
    seg = rows // SEGS
    me = lax.axis_index(SP)
    h = jnp.zeros((1, 128), F32)
    for i in range(16):
        a = e_ref[i, 0:1, :]
        b = e_ref[i, 1:2, :]
        h = jnp.where(i < me, a * h + b, h)
    half = SEGS // 2
    for s in range(SEGS):
        at = s * seg
        st = s_ref[at : at + seg, :]
        pr = p_ref[at : at + seg, :]
        states = st + pr * h
        out = (states * jax.nn.gelu(g_ref[at : at + seg, :].astype(F32), approximate=True)).astype(BF)
        h = states[seg - 1 : seg, :]
        to = (s % half) * seg
        for i in range(4):
            out_ref[2 * i + s // half, to : to + seg, :] = out


def mix_kernel(
    br_ref, w0, w1, w2, w3, v0, v1, v2, v3, r0, r1, r2, r3,
    norm_ref, also_ref, keep_ref, send_ref, full, mixed, stream,
):
    x = lax.axis_index("x")
    c = lax.axis_index("c")
    rows = br_ref.shape[1]
    for i in range(8):
        full[:, 128 * i : 128 * i + 128] = br_ref[i]
    lhs = full[...]
    total = jnp.zeros((rows, 128), F32)
    pieces = []
    for d, w, v, r in ((0, w0, v0, r0), (3, w1, v1, r1), (1, w2, v2, r2), (2, w3, v3, r3)):
        block = lax.rem(x + d, 4)
        g = r[2 * rows : 2 * rows + 16, :].astype(F32)
        for k, core, ref in ((0, c, w), (1, 1 - c, v)):
            at = pl.ds(pl.multiple_of((2 * block + core) * 256, 256), 256)
            m = 6 * k
            pieces.append(
                (
                    at,
                    r,
                    rows * k,
                    g[m : m + 1] + g[m + 1 : m + 2] + g[m + 2 : m + 3],
                    g[m + 3 : m + 4] + g[m + 4 : m + 5] + g[m + 5 : m + 6],
                )
            )
            m = jnp.dot(lhs, ref[...], preferred_element_type=F32).astype(BF)
            mixed[:, at] = m
            mf = m.astype(F32)
            mf = mf * mf
            total = total + mf[:, :128] + mf[:, 128:]
    scale = lax.rsqrt(jnp.sum(total, axis=1, keepdims=True) / 2048.0 + EPS)
    total = jnp.zeros((rows, 128), F32)
    for at, res, lo, mg, _ in pieces:
        r = res[lo : lo + rows, :].astype(F32)
        s = (r + mixed[:, at].astype(F32) * scale * mg).astype(BF)
        stream[:, at] = s
        sf = s.astype(F32)
        sf = sf * sf
        total = total + sf[:, :128] + sf[:, 128:]
    scale = lax.rsqrt(jnp.sum(total, axis=1, keepdims=True) / 2048.0 + EPS)
    for at, _, _, _, pg in pieces:
        n = (stream[:, at].astype(F32) * scale * pg).astype(BF)
        norm_ref[:, at] = n
        also_ref[:, at] = n
    keep_ref[...] = stream[:, pl.ds(pl.multiple_of((2 * x + c) * 256, 256), 256)]
    send_ref[...] = stream[:, pl.ds(pl.multiple_of((2 * x + 1 - c) * 256, 256), 256)]


def down_copies(w_ref, dn, sem):
    return [
        pltpu.make_async_copy(w_ref.at[s, pl.ds(1408, 704)], dn.at[s], sem) for s in range(16)
    ]


def down_dot(lhs, dn, d):
    first = 4 * lax.rem(lax.axis_index("x") + d, 4)
    part = jnp.concatenate([dn[first + i] for i in range(4)], axis=1)
    return jnp.dot(lhs, part, preferred_element_type=F32).astype(BF)


def ffn_kernel(oth_ref, own_hbm, w_ref, foth_ref, fown_ref, hoth, hid_ref, dn, gu, own_ref, sem):
    cuts = ((0, 128), (128, 384), (384, 704))
    groups = []
    for i, (lo, hi) in enumerate(cuts):
        groups.append(
            [
                pltpu.make_async_copy(
                    w_ref.at[s, pl.ds(base + lo, hi - lo)],
                    gu.at[s, pl.ds(base + lo, hi - lo)],
                    sem.at[i],
                )
                for s in range(16)
                for base in (0, 704)
            ]
        )
    downs = down_copies(w_ref, dn, sem.at[3])
    own_copy = pltpu.make_async_copy(own_hbm, own_ref, sem.at[4])
    for group in (groups[0], [own_copy], *groups[1:], downs):
        for cp in group:
            cp.start()
    turned = (((1,), (1,)), ((), ()))
    for (lo, hi), group in zip(cuts, groups):
        for cp in group:
            cp.wait()
        gate = jnp.concatenate([gu[s, lo:hi, :] for s in range(16)], axis=1)
        up = jnp.concatenate([gu[s, 704 + lo : 704 + hi, :] for s in range(16)], axis=1)
        for src, dst in ((oth_ref, hoth), (own_ref, hid_ref)):
            if lo == 0 and src is own_ref:
                own_copy.wait()
            g = lax.dot_general(src[...], gate, turned, preferred_element_type=F32)
            u = lax.dot_general(src[...], up, turned, preferred_element_type=F32)
            dst[:, lo:hi] = (jax.nn.silu(g) * u).astype(BF)
    for cp in downs:
        cp.wait()
    foth_ref[...] = down_dot(hoth[...], dn, 2)
    fown_ref[...] = down_dot(hid_ref[...], dn, 2)


def down_kernel(hoth_ref, hid_ref, dn, oth_ref, own_ref):
    for src, dst in ((hoth_ref, oth_ref), (hid_ref, own_ref)):
        lhs = src[...]
        for i, d in enumerate((1, 3, 0)):
            dst[i] = down_dot(lhs, dn, d)


def far_kernel(a_ref, b_ref, right_ref, left_ref):
    h = a_ref.shape[0] // 2
    total = a_ref[...].astype(F32) + b_ref[...].astype(F32)
    right_ref[...] = total[:h].astype(BF)
    left_ref[...] = total[h:].astype(BF)


def near_kernel(a_ref, b_ref, right_ref, left_ref, accr_ref, accl_ref, own_ref):
    h = a_ref.shape[1] // 2
    right_ref[...] = (a_ref[0, h:].astype(F32) + b_ref[0, h:].astype(F32)).astype(BF)
    left_ref[...] = (a_ref[1, :h].astype(F32) + b_ref[1, :h].astype(F32)).astype(BF)
    accr_ref[...] = a_ref[0, :h].astype(F32) + b_ref[0, :h].astype(F32)
    accl_ref[...] = a_ref[1, h:].astype(F32) + b_ref[1, h:].astype(F32)
    own_ref[...] = a_ref[2].astype(F32) + b_ref[2].astype(F32)


def relay_kernel(r_ref, l_ref, accr_ref, accl_ref, right_ref, left_ref):
    right_ref[...] = (r_ref[...].astype(F32) + accr_ref[...]).astype(BF)
    left_ref[...] = (l_ref[...].astype(F32) + accl_ref[...]).astype(BF)


def joined_kernel(own_ref, fl_ref, fr_ref, top_ref, bot_ref, keep_ref, send_ref, sq_ref):
    c = lax.axis_index("c")
    q = top_ref.shape[0]
    for k in range(2 * q // 64):
        lo = 64 * k
        at = slice(lo, lo + 64)
        if lo < q:
            more = fr_ref[at, :].astype(F32) + top_ref[at, :].astype(F32)
        else:
            more = fl_ref[lo - q : lo - q + 64, :].astype(F32) + bot_ref[lo - q : lo - q + 64, :].astype(F32)
        v = (own_ref[at, :] + more).astype(BF)
        for first, core in ((0, 0), (256, 1)):

            @pl.when(c == core)
            def _():
                keep_ref[at, :] = v[:, first : first + 256]

            @pl.when(c != core)
            def _():
                send_ref[at, :] = v[:, first : first + 256]

    for k in range(2 * q // 128):
        t = jnp.zeros((128, 128), F32)
        for ref in (keep_ref, send_ref):
            f = ref[128 * k : 128 * k + 128, :].astype(F32)
            f = f * f
            t = t + f[:, :128] + f[:, 128:]
        row = jnp.sum(t.T, axis=0, keepdims=True)
        for i in range(8):
            sq_ref[i, k : k + 1, :] = row


def final_kernel(keep_ref, got_ref, skeep_ref, sgot_ref, sq_ref, gain_ref, out_ref):
    c = lax.axis_index("c")
    half = keep_ref.shape[0]
    for f_ref, s_ref, core in ((keep_ref, skeep_ref, c), (got_ref, sgot_ref, 1 - c)):
        total = sq_ref[core]
        for i in range(1, 4):
            total = total + sq_ref[2 * i + core]
        scale = lax.rsqrt(total / 2048.0 + EPS)
        for k in range(half // 128):
            at = slice(128 * k, 128 * k + 128)
            col = stretch(scale[k : k + 1, :])
            for j in range(2):
                ln = slice(128 * j, 128 * j + 128)
                v = s_ref[at, ln].astype(F32) + f_ref[at, ln].astype(F32) * col * gain_ref[:, ln]
                out_ref[pl.ds(pl.multiple_of(core * half + 128 * k, 128), 128), ln] = v.astype(BF)


def call(fn, outs, specs, scratch=(), limit=8, out_spec=VM):
    return pl.pallas_call(
        fn,
        out_shape=tuple(jax.ShapeDtypeStruct(s, d) for s, d in outs),
        in_specs=list(specs),
        out_specs=tuple(out_spec for _ in outs),
        scratch_shapes=list(scratch),
        compiler_params=pltpu.CompilerParams(vmem_limit_bytes=limit << 20),
    )


def kept_in_hbm(*arrays):
    return [pltpu.with_memory_space_constraint(a, pltpu.HBM) for a in arrays]


def swapped(block):
    return lax.ppermute(block, "c", cyc(2, 1))


def steps(
    gate_branch, recur_input, doc_ids, conv_taps, gate_map, input_map, decay_level, decay_extra,
    out_weight, residual, mix_gain, pre_gain, ffn_gain, gate_weight, up_weight, down_weight,
):
    rows, width = recur_input.shape
    half = rows // 2
    c = lax.axis_index("c")

    (stacked,) = call(
        pack_kernel,
        [((2112, 128), BF)],
        [HB] * 3,
        [pltpu.VMEM((2112, 128), BF), pltpu.SemaphoreType.DMA((6,))],
        out_spec=HB,
    )(*kept_in_hbm(gate_weight.T, up_weight.T, down_weight))
    (weights,) = kept_in_hbm(lax.all_gather(stacked, SP, axis=0))

    res_keep = lax.dynamic_slice_in_dim(residual, c * half, half, 0)
    res_send = lax.dynamic_slice_in_dim(residual, (1 - c) * half, half, 0)
    rest = jnp.stack([mix_gain, pre_gain])
    levels = []
    for _ in range(3):
        levels.append(lax.reduce_precision(rest, 8, 7))
        rest = rest - levels[-1]
    coded = jnp.stack(levels, axis=1).reshape(6, 256).astype(BF)
    coded = jnp.concatenate([coded, swapped(coded), jnp.zeros((4, 256), BF)])
    res = jnp.concatenate([res_keep, swapped(res_send), coded])
    out_left = lax.ppermute(out_weight, "x", cyc(4, 1))
    res_right = lax.ppermute(res, "x", cyc(4, 3))
    res_left = lax.ppermute(res, "x", cyc(4, 1))
    out_right = lax.ppermute(out_weight, "x", cyc(4, 3))

    tail = jnp.pad(recur_input[rows - 3 :].astype(F32), ((5, 0), (0, 0)))
    tail_ids = jnp.pad(
        jnp.broadcast_to(doc_ids[rows - 3 :].astype(F32)[:, None], (3, width)), ((5, 0), (0, 0))
    )
    rim = lax.ppermute(
        jnp.concatenate([tail, tail_ids]), SP, [(i, i + 1) for i in range(15)]
    )
    nsp = (-8.0 * jax.nn.softplus(-decay_level))[None, :]
    states, products, ends = call(
        scan_kernel,
        [((rows, width), F32), ((rows, width), F32), ((16, 2, width), F32)],
        [VM] * 8,
        [
            pltpu.VMEM((rows + 8, width), F32),
            pltpu.VMEM((rows + 8, width), F32),
            pltpu.VMEM((rows, width), F32),
            pltpu.VMEM((rows, width), F32),
        ],
    )(
        *kept_in_hbm(recur_input),
        rim,
        doc_ids.astype(F32).reshape(rows // 128, 128),
        *kept_in_hbm(conv_taps, gate_map, input_map),
        nsp,
        *kept_in_hbm(decay_extra),
    )
    all_ends = lax.all_to_all(ends, SP, 0, 0, tiled=True)
    (branch,) = call(branch_kernel, [((8, half, width), BF)], [VM] * 4)(
        states, products, all_ends, *kept_in_hbm(gate_branch)
    )
    branch = lax.all_to_all(branch, TP, 0, 0, tiled=True)
    out_far = lax.ppermute(out_left, "x", cyc(4, 1))
    res_far = lax.ppermute(res_right, "x", cyc(4, 3))
    outs = [out_weight, out_left, out_right]
    others = [swapped(b) for b in outs]
    others.append(swapped(out_far))
    outs.append(out_far)
    norm_send, norm_own, skeep, ssend = call(
        mix_kernel,
        [((half, 2048), BF)] * 2 + [((half, 256), BF)] * 2,
        [VM] * 13,
        [
            pltpu.VMEM((half, 1024), BF),
            pltpu.VMEM((half, 2048), BF),
            pltpu.VMEM((half, 2048), BF),
        ],
        limit=12,
    )(branch, *outs, *others, res, res_left, res_right, res_far)
    (norm_own,) = kept_in_hbm(norm_own)
    norm_oth = swapped(norm_send)
    sgot = swapped(ssend)

    far_oth, far_own, hid_oth, hid_own, down = call(
        ffn_kernel,
        [((half, 512), BF)] * 2 + [((half, 704), BF)] * 2 + [((16, 704, 128), BF)],
        [VM, HB, HB],
        [
            pltpu.VMEM((16, 1408, 128), BF),
            pltpu.VMEM((half, 2048), BF),
            pltpu.SemaphoreType.DMA((5,)),
        ],
        limit=17,
    )(norm_oth, norm_own, weights)
    far_in = swapped(far_oth)
    rest_oth, rest_own = call(
        down_kernel, [((3, half, 512), BF)] * 2, [VM] * 3, limit=14
    )(hid_oth, hid_own, down)
    rest_in = swapped(rest_oth)
    q = half // 2
    far_r, far_l = call(far_kernel, [((q, 512), BF)] * 2, [VM] * 2)(far_own, far_in)
    pass_r = lax.ppermute(far_r, "x", cyc(4, 1))
    pass_l = lax.ppermute(far_l, "x", cyc(4, 3))
    near_r, near_l, acc_r, acc_l, own = call(
        near_kernel,
        [((q, 512), BF)] * 2 + [((q, 512), F32)] * 2 + [((half, 512), F32)],
        [VM] * 2,
        limit=10,
    )(rest_own, rest_in)
    from_left = lax.ppermute(near_r, "x", cyc(4, 1))
    from_right = lax.ppermute(near_l, "x", cyc(4, 3))
    pass_r, pass_l = lax.optimization_barrier((pass_r, pass_l))
    right2, left2 = call(relay_kernel, [((q, 512), BF)] * 2, [VM] * 4)(pass_r, pass_l, acc_r, acc_l)
    top = lax.ppermute(right2, "x", cyc(4, 1))
    bottom = lax.ppermute(left2, "x", cyc(4, 3))
    from_left, from_right, top, bottom = lax.optimization_barrier(
        (from_left, from_right, top, bottom)
    )
    fkeep, fsend, square = call(
        joined_kernel,
        [((half, 256), BF)] * 2 + [((8, 3, 128), F32)],
        [VM] * 5,
    )(own, from_left, from_right, top, bottom)
    fgot = swapped(fsend)
    square = lax.all_to_all(square, TP, 0, 0, tiled=True)
    (out,) = call(final_kernel, [((rows, 256), BF)], [VM] * 6)(
        fkeep, fgot, skeep, sgot, square, ffn_gain[None, :]
    )
    return out


def solution(mesh):
    split = Mesh(mesh.devices.reshape(4, 4, 4, 2), ("z", "y", "x", "c"))
    return jax.shard_map(
        steps,
        mesh=split,
        in_specs=(
            P(SP, TP), P(SP, TP), P(SP), P(None, TP), P(TP, None, None), P(TP, None, None), P(TP),
            P(SP, TP), P(None, TP), P(SP, TP), P(TP), P(TP), P(TP), P(SP, TP), P(SP, TP), P(TP, SP),
        ),
        out_specs=P(SP, TP),
        check_vma=False,
    )
```

```python
import jax
import jax.numpy as jnp
from jax import lax
from jax.experimental import pallas as pl
from jax.experimental.pallas import tpu as pltpu
from jax.sharding import Mesh
from jax.sharding import PartitionSpec as P

SP = ("z", "y")
TP = ("x", "c")
EPS = 1e-06
BF = jnp.bfloat16
F32 = jnp.float32
VM = pl.BlockSpec(memory_space=pltpu.VMEM)
HB = pl.BlockSpec(memory_space=pltpu.HBM)
SEGS = 8


def cyc(count, step):
    return [(i, (i + step) % count) for i in range(count)]


def stretch(row, lanes=128):
    return jnp.broadcast_to(row, (lanes, 128)).T


def taylor_expm1_neg(y):
    p = 1.0 + y * (1.0 / 8.0)
    for k in (7.0, 6.0, 5.0, 4.0, 3.0, 2.0):
        p = 1.0 + y * (1.0 / k) * p
    return -y * p


def pack_kernel(g_ref, u_ref, d_ref, out_ref, buf, sem):
    spans = [pl.ds(704 * i, 704) for i in range(3)]
    fetches = [
        pltpu.make_async_copy(ref, buf.at[span], sem.at[i])
        for i, (ref, span) in enumerate(zip((g_ref, u_ref, d_ref), spans))
    ]
    stores = [
        pltpu.make_async_copy(buf.at[span], out_ref.at[span], sem.at[3 + i])
        for i, span in enumerate(spans)
    ]
    for cp in fetches:
        cp.start()
    for cp, then in zip(fetches, stores):
        cp.wait()
        then.start()
    for cp in stores:
        cp.wait()


def scan_kernel(
    x_ref, rim_ref, ids_ref, taps_ref, gm_ref, im_ref, nsp_ref, extra_ref,
    s_ref, p_ref, e_ref, xs, idx, fs, ds,
):
    rows = x_ref.shape[0]
    taps = taps_ref[...].astype(F32)
    head = gm_ref.shape[1]

    def blockdiag(ref):
        zero = jnp.zeros((head, head), BF)
        return jnp.concatenate(
            [
                jnp.concatenate([ref[0], zero], axis=1),
                jnp.concatenate([zero, ref[1]], axis=1),
            ],
            axis=0,
        )

    gate = blockdiag(gm_ref)
    inp = blockdiag(im_ref)
    xs[0:8, :] = rim_ref[0:8, :]
    idx[0:8, :] = rim_ref[8:16, :]
    for j in range(rows // 128):
        at = 8 + 128 * j
        xs[at : at + 128, :] = x_ref[128 * j : 128 * j + 128, :].astype(F32)
        idx[at : at + 128, :] = stretch(ids_ref[j : j + 1, :])
    for j in range(rows // 128):
        at = 8 + 128 * j
        here = idx[at : at + 128, :]
        before = idx[at - 1 : at + 127, :]
        conv = xs[at : at + 128, :] * taps[0:1, :]
        for k in range(1, 4):
            old = idx[at - k : at - k + 128, :]
            conv = conv + jnp.where(old == here, xs[at - k : at - k + 128, :], 0.0) * taps[k : k + 1, :]
        conv = conv.astype(BF)
        rg = jax.nn.sigmoid(jnp.dot(conv, gate, preferred_element_type=F32))
        ig = jax.nn.sigmoid(jnp.dot(conv, inp, preferred_element_type=F32))
        ld = nsp_ref[...] * rg + extra_ref[128 * j : 128 * j + 128, :]
        e = jnp.exp(ld)
        y = 2.0 * ld
        em = jnp.where(y > -0.5, taylor_expm1_neg(jnp.maximum(y, -0.5)), 1.0 - e * e)
        fs[128 * j : 128 * j + 128, :] = jnp.where(before == here, e, 0.0)
        ds[128 * j : 128 * j + 128, :] = jnp.sqrt(em) * ig * conv.astype(F32)
    seg = rows // SEGS

    def step(j, carry):
        h, p = carry
        f = fs[pl.ds(j, SEGS, stride=seg), :]
        d = ds[pl.ds(j, SEGS, stride=seg), :]
        h = f * h + d
        p = p * f
        s_ref[pl.ds(j, SEGS, stride=seg), :] = h
        p_ref[pl.ds(j, SEGS, stride=seg), :] = p
        return h, p

    zero = jnp.zeros((SEGS, 128), F32)
    h, p = lax.fori_loop(0, seg, step, (zero, zero + 1.0), unroll=8)
    a = p[0:1, :]
    b = h[0:1, :]
    for s in range(1, SEGS):
        b = p[s : s + 1, :] * b + h[s : s + 1, :]
        a = p[s : s + 1, :] * a
    for i in range(16):
        e_ref[i, 0:1, :] = a
        e_ref[i, 1:2, :] = b


def branch_kernel(s_ref, p_ref, e_ref, g_ref, out_ref):
    rows = s_ref.shape[0]
    seg = rows // SEGS
    me = lax.axis_index(SP)
    h = jnp.zeros((1, 128), F32)
    for i in range(16):
        a = e_ref[i, 0:1, :]
        b = e_ref[i, 1:2, :]
        h = jnp.where(i < me, a * h + b, h)
    half = SEGS // 2
    for s in range(SEGS):
        at = s * seg
        st = s_ref[at : at + seg, :]
        pr = p_ref[at : at + seg, :]
        states = st + pr * h
        out = (states * jax.nn.gelu(g_ref[at : at + seg, :].astype(F32), approximate=True)).astype(BF)
        h = states[seg - 1 : seg, :]
        to = (s % half) * seg
        for i in range(4):
            out_ref[2 * i + s // half, to : to + seg, :] = out


def mix_kernel(
    br_ref, w0, w1, w2, w3, v0, v1, v2, v3, r0, r1, r2, r3,
    norm_ref, also_ref, keep_ref, send_ref, full, mixed, stream,
):
    x = lax.axis_index("x")
    c = lax.axis_index("c")
    rows = br_ref.shape[1]
    for i in range(8):
        full[:, 128 * i : 128 * i + 128] = br_ref[i]
    lhs = full[...]
    total = jnp.zeros((rows, 128), F32)
    pieces = []
    for d, w, v, r in ((0, w0, v0, r0), (3, w1, v1, r1), (1, w2, v2, r2), (2, w3, v3, r3)):
        block = lax.rem(x + d, 4)
        g = r[2 * rows : 2 * rows + 16, :].astype(F32)
        for k, core, ref in ((0, c, w), (1, 1 - c, v)):
            at = pl.ds(pl.multiple_of((2 * block + core) * 256, 256), 256)
            m = 6 * k
            pieces.append(
                (
                    at,
                    r,
                    rows * k,
                    g[m : m + 1] + g[m + 1 : m + 2] + g[m + 2 : m + 3],
                    g[m + 3 : m + 4] + g[m + 4 : m + 5] + g[m + 5 : m + 6],
                )
            )
            m = jnp.dot(lhs, ref[...], preferred_element_type=F32).astype(BF)
            mixed[:, at] = m
            mf = m.astype(F32)
            mf = mf * mf
            total = total + mf[:, :128] + mf[:, 128:]
    scale = lax.rsqrt(jnp.sum(total, axis=1, keepdims=True) / 2048.0 + EPS)
    total = jnp.zeros((rows, 128), F32)
    for at, res, lo, mg, _ in pieces:
        r = res[lo : lo + rows, :].astype(F32)
        s = (r + mixed[:, at].astype(F32) * scale * mg).astype(BF)
        stream[:, at] = s
        sf = s.astype(F32)
        sf = sf * sf
        total = total + sf[:, :128] + sf[:, 128:]
    scale = lax.rsqrt(jnp.sum(total, axis=1, keepdims=True) / 2048.0 + EPS)
    for at, _, _, _, pg in pieces:
        n = (stream[:, at].astype(F32) * scale * pg).astype(BF)
        norm_ref[:, at] = n
        also_ref[:, at] = n
    keep_ref[...] = stream[:, pl.ds(pl.multiple_of((2 * x + c) * 256, 256), 256)]
    send_ref[...] = stream[:, pl.ds(pl.multiple_of((2 * x + 1 - c) * 256, 256), 256)]


def down_dot(lhs, dn, d):
    first = 4 * lax.rem(lax.axis_index("x") + d, 4)
    part = jnp.concatenate([dn[first + i] for i in range(4)], axis=1)
    return jnp.dot(lhs, part, preferred_element_type=F32).astype(BF)


CUTS = ((0, 128), (128, 384), (384, 704))


def hidden_part(src, gu, lo, hi):
    turned = (((1,), (1,)), ((), ()))
    gate = jnp.concatenate([gu[s, lo:hi, :] for s in range(16)], axis=1)
    up = jnp.concatenate([gu[s, 704 + lo : 704 + hi, :] for s in range(16)], axis=1)
    g = lax.dot_general(src, gate, turned, preferred_element_type=F32)
    u = lax.dot_general(src, up, turned, preferred_element_type=F32)
    return (jax.nn.silu(g) * u).astype(BF)


def first_kernel(n_ref, own_hbm, w_ref, far_ref, rest_ref, gu, dn, own_ref, hid, sem):
    groups = []
    for i, (lo, hi) in enumerate(CUTS):
        groups.append(
            [
                pltpu.make_async_copy(
                    w_ref.at[s, pl.ds(base + lo, hi - lo)],
                    gu.at[s, pl.ds(base + lo, hi - lo)],
                    sem.at[i],
                )
                for s in range(16)
                for base in (0, 704)
            ]
        )
    downs = [
        pltpu.make_async_copy(w_ref.at[s, pl.ds(1408, 704)], dn.at[s], sem.at[3]) for s in range(16)
    ]
    own_copy = pltpu.make_async_copy(own_hbm, own_ref, sem.at[4])
    for group in groups + [downs, [own_copy]]:
        for cp in group:
            cp.start()
    for (lo, hi), group in zip(CUTS, groups):
        for cp in group:
            cp.wait()
        hid[:, lo:hi] = hidden_part(n_ref[...], gu, lo, hi)
    for cp in downs:
        cp.wait()
    lhs = hid[...]
    far_ref[...] = down_dot(lhs, dn, 2)
    for i, d in enumerate((1, 3, 0)):
        rest_ref[i] = down_dot(lhs, dn, d)
    own_copy.wait()


def second_kernel(n_ref, gu, dn, far_ref, hid_ref):
    for lo, hi in CUTS:
        hid_ref[:, lo:hi] = hidden_part(n_ref[...], gu, lo, hi)
    far_ref[...] = down_dot(hid_ref[...], dn, 2)


def third_kernel(hid_ref, dn, rest_ref):
    lhs = hid_ref[...]
    for i, d in enumerate((1, 3, 0)):
        rest_ref[i] = down_dot(lhs, dn, d)


def far_kernel(a_ref, b_ref, right_ref, left_ref):
    h = a_ref.shape[0] // 2
    total = a_ref[...].astype(F32) + b_ref[...].astype(F32)
    right_ref[...] = total[:h].astype(BF)
    left_ref[...] = total[h:].astype(BF)


def near_kernel(a_ref, b_ref, right_ref, left_ref, accr_ref, accl_ref, own_ref):
    h = a_ref.shape[1] // 2
    right_ref[...] = (a_ref[0, h:].astype(F32) + b_ref[0, h:].astype(F32)).astype(BF)
    left_ref[...] = (a_ref[1, :h].astype(F32) + b_ref[1, :h].astype(F32)).astype(BF)
    accr_ref[...] = a_ref[0, :h].astype(F32) + b_ref[0, :h].astype(F32)
    accl_ref[...] = a_ref[1, h:].astype(F32) + b_ref[1, h:].astype(F32)
    own_ref[...] = a_ref[2].astype(F32) + b_ref[2].astype(F32)


def relay_kernel(r_ref, l_ref, accr_ref, accl_ref, right_ref, left_ref):
    right_ref[...] = (r_ref[...].astype(F32) + accr_ref[...]).astype(BF)
    left_ref[...] = (l_ref[...].astype(F32) + accl_ref[...]).astype(BF)


def joined_kernel(own_ref, fl_ref, fr_ref, top_ref, bot_ref, keep_ref, send_ref, sq_ref):
    c = lax.axis_index("c")
    q = top_ref.shape[0]
    for k in range(2 * q // 64):
        lo = 64 * k
        at = slice(lo, lo + 64)
        if lo < q:
            more = fr_ref[at, :].astype(F32) + top_ref[at, :].astype(F32)
        else:
            more = fl_ref[lo - q : lo - q + 64, :].astype(F32) + bot_ref[lo - q : lo - q + 64, :].astype(F32)
        v = (own_ref[at, :] + more).astype(BF)
        for first, core in ((0, 0), (256, 1)):

            @pl.when(c == core)
            def _():
                keep_ref[at, :] = v[:, first : first + 256]

            @pl.when(c != core)
            def _():
                send_ref[at, :] = v[:, first : first + 256]

    for k in range(2 * q // 128):
        t = jnp.zeros((128, 128), F32)
        for ref in (keep_ref, send_ref):
            f = ref[128 * k : 128 * k + 128, :].astype(F32)
            f = f * f
            t = t + f[:, :128] + f[:, 128:]
        row = jnp.sum(t.T, axis=0, keepdims=True)
        for i in range(8):
            sq_ref[i, k : k + 1, :] = row


def final_kernel(keep_ref, got_ref, skeep_ref, sgot_ref, sq_ref, gain_ref, out_ref):
    c = lax.axis_index("c")
    half = keep_ref.shape[0]
    for f_ref, s_ref, core in ((keep_ref, skeep_ref, c), (got_ref, sgot_ref, 1 - c)):
        total = sq_ref[core]
        for i in range(1, 4):
            total = total + sq_ref[2 * i + core]
        scale = lax.rsqrt(total / 2048.0 + EPS)
        for k in range(half // 128):
            at = slice(128 * k, 128 * k + 128)
            col = stretch(scale[k : k + 1, :])
            for j in range(2):
                ln = slice(128 * j, 128 * j + 128)
                v = s_ref[at, ln].astype(F32) + f_ref[at, ln].astype(F32) * col * gain_ref[:, ln]
                out_ref[pl.ds(pl.multiple_of(core * half + 128 * k, 128), 128), ln] = v.astype(BF)


def call(fn, outs, specs, scratch=(), limit=8, out_spec=VM):
    return pl.pallas_call(
        fn,
        out_shape=tuple(jax.ShapeDtypeStruct(s, d) for s, d in outs),
        in_specs=list(specs),
        out_specs=tuple(out_spec for _ in outs),
        scratch_shapes=list(scratch),
        compiler_params=pltpu.CompilerParams(vmem_limit_bytes=limit << 20),
    )


def kept_in_hbm(*arrays):
    return [pltpu.with_memory_space_constraint(a, pltpu.HBM) for a in arrays]


def swapped(block):
    return lax.ppermute(block, "c", cyc(2, 1))


def steps(
    gate_branch, recur_input, doc_ids, conv_taps, gate_map, input_map, decay_level, decay_extra,
    out_weight, residual, mix_gain, pre_gain, ffn_gain, gate_weight, up_weight, down_weight,
):
    rows, width = recur_input.shape
    half = rows // 2
    c = lax.axis_index("c")

    (stacked,) = call(
        pack_kernel,
        [((2112, 128), BF)],
        [HB] * 3,
        [pltpu.VMEM((2112, 128), BF), pltpu.SemaphoreType.DMA((6,))],
        out_spec=HB,
    )(*kept_in_hbm(gate_weight.T, up_weight.T, down_weight))
    (weights,) = kept_in_hbm(lax.all_gather(stacked, SP, axis=0))

    res_keep = lax.dynamic_slice_in_dim(residual, c * half, half, 0)
    res_send = lax.dynamic_slice_in_dim(residual, (1 - c) * half, half, 0)
    rest = jnp.stack([mix_gain, pre_gain])
    levels = []
    for _ in range(3):
        levels.append(lax.reduce_precision(rest, 8, 7))
        rest = rest - levels[-1]
    coded = jnp.stack(levels, axis=1).reshape(6, 256).astype(BF)
    coded = jnp.concatenate([coded, swapped(coded), jnp.zeros((4, 256), BF)])
    res = jnp.concatenate([res_keep, swapped(res_send), coded])
    out_left = lax.ppermute(out_weight, "x", cyc(4, 1))
    res_right = lax.ppermute(res, "x", cyc(4, 3))
    res_left = lax.ppermute(res, "x", cyc(4, 1))
    out_right = lax.ppermute(out_weight, "x", cyc(4, 3))

    tail = jnp.pad(recur_input[rows - 3 :].astype(F32), ((5, 0), (0, 0)))
    tail_ids = jnp.pad(
        jnp.broadcast_to(doc_ids[rows - 3 :].astype(F32)[:, None], (3, width)), ((5, 0), (0, 0))
    )
    rim = lax.ppermute(
        jnp.concatenate([tail, tail_ids]), SP, [(i, i + 1) for i in range(15)]
    )
    nsp = (-8.0 * jax.nn.softplus(-decay_level))[None, :]
    states, products, ends = call(
        scan_kernel,
        [((rows, width), F32), ((rows, width), F32), ((16, 2, width), F32)],
        [VM] * 8,
        [
            pltpu.VMEM((rows + 8, width), F32),
            pltpu.VMEM((rows + 8, width), F32),
            pltpu.VMEM((rows, width), F32),
            pltpu.VMEM((rows, width), F32),
        ],
    )(
        *kept_in_hbm(recur_input),
        rim,
        doc_ids.astype(F32).reshape(rows // 128, 128),
        *kept_in_hbm(conv_taps, gate_map, input_map),
        nsp,
        *kept_in_hbm(decay_extra),
    )
    all_ends = lax.all_to_all(ends, SP, 0, 0, tiled=True)
    (branch,) = call(branch_kernel, [((8, half, width), BF)], [VM] * 4)(
        states, products, all_ends, *kept_in_hbm(gate_branch)
    )
    branch = lax.all_to_all(branch, TP, 0, 0, tiled=True)
    out_far = lax.ppermute(out_left, "x", cyc(4, 1))
    res_far = lax.ppermute(res_right, "x", cyc(4, 3))
    outs = [out_weight, out_left, out_right]
    others = [swapped(b) for b in outs]
    others.append(swapped(out_far))
    outs.append(out_far)
    norm_send, norm_own, skeep, ssend = call(
        mix_kernel,
        [((half, 2048), BF)] * 2 + [((half, 256), BF)] * 2,
        [VM] * 13,
        [
            pltpu.VMEM((half, 1024), BF),
            pltpu.VMEM((half, 2048), BF),
            pltpu.VMEM((half, 2048), BF),
        ],
        limit=12,
    )(branch, *outs, *others, res, res_left, res_right, res_far)
    (norm_own,) = kept_in_hbm(norm_own)
    norm_oth = swapped(norm_send)
    sgot = swapped(ssend)

    far_oth, rest_oth, gate_up, down, norm_own = call(
        first_kernel,
        [
            ((half, 512), BF),
            ((3, half, 512), BF),
            ((16, 1408, 128), BF),
            ((16, 704, 128), BF),
            ((half, 2048), BF),
        ],
        [VM, HB, HB],
        [pltpu.VMEM((half, 704), BF), pltpu.SemaphoreType.DMA((5,))],
        limit=18,
    )(norm_oth, norm_own, weights)
    far_in = swapped(far_oth)
    rest_in = swapped(rest_oth)
    far_own, hid_own = call(
        second_kernel, [((half, 512), BF), ((half, 704), BF)], [VM] * 3, limit=18
    )(norm_own, gate_up, down)
    (rest_own,) = call(third_kernel, [((3, half, 512), BF)], [VM] * 2, limit=14)(hid_own, down)
    q = half // 2
    far_r, far_l = call(far_kernel, [((q, 512), BF)] * 2, [VM] * 2)(far_own, far_in)
    pass_r = lax.ppermute(far_r, "x", cyc(4, 1))
    pass_l = lax.ppermute(far_l, "x", cyc(4, 3))
    near_r, near_l, acc_r, acc_l, own = call(
        near_kernel,
        [((q, 512), BF)] * 2 + [((q, 512), F32)] * 2 + [((half, 512), F32)],
        [VM] * 2,
        limit=10,
    )(rest_own, rest_in)
    from_left = lax.ppermute(near_r, "x", cyc(4, 1))
    from_right = lax.ppermute(near_l, "x", cyc(4, 3))
    pass_r, pass_l = lax.optimization_barrier((pass_r, pass_l))
    right2, left2 = call(relay_kernel, [((q, 512), BF)] * 2, [VM] * 4)(pass_r, pass_l, acc_r, acc_l)
    top = lax.ppermute(right2, "x", cyc(4, 1))
    bottom = lax.ppermute(left2, "x", cyc(4, 3))
    from_left, from_right, top, bottom = lax.optimization_barrier(
        (from_left, from_right, top, bottom)
    )
    fkeep, fsend, square = call(
        joined_kernel,
        [((half, 256), BF)] * 2 + [((8, 3, 128), F32)],
        [VM] * 5,
    )(own, from_left, from_right, top, bottom)
    fgot = swapped(fsend)
    square = lax.all_to_all(square, TP, 0, 0, tiled=True)
    (out,) = call(final_kernel, [((rows, 256), BF)], [VM] * 6)(
        fkeep, fgot, skeep, sgot, square, ffn_gain[None, :]
    )
    return out


def solution(mesh):
    split = Mesh(mesh.devices.reshape(4, 4, 4, 2), ("z", "y", "x", "c"))
    return jax.shard_map(
        steps,
        mesh=split,
        in_specs=(
            P(SP, TP), P(SP, TP), P(SP), P(None, TP), P(TP, None, None), P(TP, None, None), P(TP),
            P(SP, TP), P(None, TP), P(SP, TP), P(TP), P(TP), P(TP), P(SP, TP), P(SP, TP), P(TP, SP),
        ),
        out_specs=P(SP, TP),
        check_vma=False,
    )
```

```python
import jax
import jax.numpy as jnp
from jax import lax
from jax.experimental import pallas as pl
from jax.experimental.pallas import tpu as pltpu
from jax.sharding import Mesh
from jax.sharding import PartitionSpec as P

SP = ("z", "y")
TP = ("x", "c")
EPS = 1e-06
BF = jnp.bfloat16
F32 = jnp.float32
VM = pl.BlockSpec(memory_space=pltpu.VMEM)
HB = pl.BlockSpec(memory_space=pltpu.HBM)
SEGS = 8


def cyc(count, step):
    return [(i, (i + step) % count) for i in range(count)]


def stretch(row, lanes=128):
    return jnp.broadcast_to(row, (lanes, 128)).T


def taylor_expm1_neg(y):
    p = 1.0 + y * (1.0 / 8.0)
    for k in (7.0, 6.0, 5.0, 4.0, 3.0, 2.0):
        p = 1.0 + y * (1.0 / k) * p
    return -y * p


def pack_kernel(g_ref, u_ref, d_ref, out_ref, buf, sem):
    spans = [pl.ds(704 * i, 704) for i in range(3)]
    fetches = [
        pltpu.make_async_copy(ref, buf.at[span], sem.at[i])
        for i, (ref, span) in enumerate(zip((g_ref, u_ref, d_ref), spans))
    ]
    stores = [
        pltpu.make_async_copy(buf.at[span], out_ref.at[span], sem.at[3 + i])
        for i, span in enumerate(spans)
    ]
    for cp in fetches:
        cp.start()
    for cp, then in zip(fetches, stores):
        cp.wait()
        then.start()
    for cp in stores:
        cp.wait()


def scan_kernel(
    x_ref, rim_ref, ids_ref, taps_ref, gm_ref, im_ref, nsp_ref, extra_ref,
    s_ref, p_ref, e_ref, xs, idx, fs, ds,
):
    rows = x_ref.shape[0]
    taps = taps_ref[...].astype(F32)
    head = gm_ref.shape[1]

    def blockdiag(ref):
        zero = jnp.zeros((head, head), BF)
        return jnp.concatenate(
            [
                jnp.concatenate([ref[0], zero], axis=1),
                jnp.concatenate([zero, ref[1]], axis=1),
            ],
            axis=0,
        )

    gate = blockdiag(gm_ref)
    inp = blockdiag(im_ref)
    xs[0:8, :] = rim_ref[0:8, :]
    idx[0:8, :] = rim_ref[8:16, :]
    for j in range(rows // 128):
        at = 8 + 128 * j
        xs[at : at + 128, :] = x_ref[128 * j : 128 * j + 128, :].astype(F32)
        idx[at : at + 128, :] = stretch(ids_ref[j : j + 1, :])
    for j in range(rows // 128):
        at = 8 + 128 * j
        here = idx[at : at + 128, :]
        before = idx[at - 1 : at + 127, :]
        conv = xs[at : at + 128, :] * taps[0:1, :]
        for k in range(1, 4):
            old = idx[at - k : at - k + 128, :]
            conv = conv + jnp.where(old == here, xs[at - k : at - k + 128, :], 0.0) * taps[k : k + 1, :]
        conv = conv.astype(BF)
        rg = jax.nn.sigmoid(jnp.dot(conv, gate, preferred_element_type=F32))
        ig = jax.nn.sigmoid(jnp.dot(conv, inp, preferred_element_type=F32))
        ld = nsp_ref[...] * rg + extra_ref[128 * j : 128 * j + 128, :]
        e = jnp.exp(ld)
        y = 2.0 * ld
        em = jnp.where(y > -0.5, taylor_expm1_neg(jnp.maximum(y, -0.5)), 1.0 - e * e)
        fs[128 * j : 128 * j + 128, :] = jnp.where(before == here, e, 0.0)
        ds[128 * j : 128 * j + 128, :] = jnp.sqrt(em) * ig * conv.astype(F32)
    seg = rows // SEGS

    def step(j, carry):
        h, p = carry
        f = fs[pl.ds(j, SEGS, stride=seg), :]
        d = ds[pl.ds(j, SEGS, stride=seg), :]
        h = f * h + d
        p = p * f
        s_ref[pl.ds(j, SEGS, stride=seg), :] = h
        p_ref[pl.ds(j, SEGS, stride=seg), :] = p
        return h, p

    zero = jnp.zeros((SEGS, 128), F32)
    h, p = lax.fori_loop(0, seg, step, (zero, zero + 1.0), unroll=8)
    a = p[0:1, :]
    b = h[0:1, :]
    for s in range(1, SEGS):
        b = p[s : s + 1, :] * b + h[s : s + 1, :]
        a = p[s : s + 1, :] * a
    for i in range(16):
        e_ref[i, 0:1, :] = a
        e_ref[i, 1:2, :] = b


def branch_kernel(s_ref, p_ref, e_ref, g_ref, out_ref):
    rows = s_ref.shape[0]
    seg = rows // SEGS
    me = lax.axis_index(SP)
    h = jnp.zeros((1, 128), F32)
    for i in range(16):
        a = e_ref[i, 0:1, :]
        b = e_ref[i, 1:2, :]
        h = jnp.where(i < me, a * h + b, h)
    half = SEGS // 2
    for s in range(SEGS):
        at = s * seg
        st = s_ref[at : at + seg, :]
        pr = p_ref[at : at + seg, :]
        states = st + pr * h
        out = (states * jax.nn.gelu(g_ref[at : at + seg, :].astype(F32), approximate=True)).astype(BF)
        h = states[seg - 1 : seg, :]
        to = (s % half) * seg
        for i in range(4):
            out_ref[2 * i + s // half, to : to + seg, :] = out


def mix_kernel(
    br_ref, w0, w1, w2, w3, v0, v1, v2, v3, r0, r1, r2, r3,
    norm_ref, also_ref, keep_ref, send_ref, full, mixed, stream,
):
    x = lax.axis_index("x")
    c = lax.axis_index("c")
    rows = br_ref.shape[1]
    for i in range(8):
        full[:, 128 * i : 128 * i + 128] = br_ref[i]
    lhs = full[...]
    total = jnp.zeros((rows, 128), F32)
    pieces = []
    for d, w, v, r in ((0, w0, v0, r0), (3, w1, v1, r1), (1, w2, v2, r2), (2, w3, v3, r3)):
        block = lax.rem(x + d, 4)
        g = r[2 * rows : 2 * rows + 16, :].astype(F32)
        for k, core, ref in ((0, c, w), (1, 1 - c, v)):
            at = pl.ds(pl.multiple_of((2 * block + core) * 256, 256), 256)
            m = 6 * k
            pieces.append(
                (
                    at,
                    r,
                    rows * k,
                    g[m : m + 1] + g[m + 1 : m + 2] + g[m + 2 : m + 3],
                    g[m + 3 : m + 4] + g[m + 4 : m + 5] + g[m + 5 : m + 6],
                )
            )
            m = jnp.dot(lhs, ref[...], preferred_element_type=F32).astype(BF)
            mixed[:, at] = m
            mf = m.astype(F32)
            mf = mf * mf
            total = total + mf[:, :128] + mf[:, 128:]
    scale = lax.rsqrt(jnp.sum(total, axis=1, keepdims=True) / 2048.0 + EPS)
    total = jnp.zeros((rows, 128), F32)
    for at, res, lo, mg, _ in pieces:
        r = res[lo : lo + rows, :].astype(F32)
        s = (r + mixed[:, at].astype(F32) * scale * mg).astype(BF)
        stream[:, at] = s
        sf = s.astype(F32)
        sf = sf * sf
        total = total + sf[:, :128] + sf[:, 128:]
    scale = lax.rsqrt(jnp.sum(total, axis=1, keepdims=True) / 2048.0 + EPS)
    for at, _, _, _, pg in pieces:
        n = (stream[:, at].astype(F32) * scale * pg).astype(BF)
        norm_ref[:, at] = n
        also_ref[:, at] = n
    keep_ref[...] = stream[:, pl.ds(pl.multiple_of((2 * x + c) * 256, 256), 256)]
    send_ref[...] = stream[:, pl.ds(pl.multiple_of((2 * x + 1 - c) * 256, 256), 256)]


def down_dot(lhs, dn, d):
    first = 4 * lax.rem(lax.axis_index("x") + d, 4)
    part = jnp.concatenate([dn[first + i] for i in range(4)], axis=1)
    return jnp.dot(lhs, part, preferred_element_type=F32).astype(BF)


CUTS = ((0, 128), (128, 384), (384, 704))


def hidden_part(src, gu, lo, hi):
    rows = [
        jnp.concatenate([gu[s, base + lo : base + hi, :] for s in range(16)], axis=1)
        for base in (0, 704)
    ]
    act = lax.dot_general(
        src, jnp.concatenate(rows), (((1,), (1,)), ((), ())), preferred_element_type=F32
    )
    return (jax.nn.silu(act[:, : hi - lo]) * act[:, hi - lo :]).astype(BF)


def first_kernel(n_ref, own_hbm, w_ref, far_ref, rest_ref, gu, dn, own_ref, hid, sem):
    groups = []
    for i, (lo, hi) in enumerate(CUTS):
        groups.append(
            [
                pltpu.make_async_copy(
                    w_ref.at[s, pl.ds(base + lo, hi - lo)],
                    gu.at[s, pl.ds(base + lo, hi - lo)],
                    sem.at[i],
                )
                for s in range(16)
                for base in (0, 704)
            ]
        )
    downs = [
        pltpu.make_async_copy(w_ref.at[s, pl.ds(1408, 704)], dn.at[s], sem.at[4]) for s in range(16)
    ]
    own_copy = pltpu.make_async_copy(own_hbm, own_ref, sem.at[5])
    for group in groups + [downs, [own_copy]]:
        for cp in group:
            cp.start()
    for (lo, hi), group in zip(CUTS, groups):
        for cp in group:
            cp.wait()
        hid[:, lo:hi] = hidden_part(n_ref[...], gu, lo, hi)
    for cp in downs:
        cp.wait()
    lhs = hid[...]
    far_ref[...] = down_dot(lhs, dn, 2)
    for i, d in enumerate((1, 3, 0)):
        rest_ref[i] = down_dot(lhs, dn, d)
    own_copy.wait()


def second_kernel(n_ref, gu, dn, far_ref, hid_ref):
    for lo, hi in CUTS:
        hid_ref[:, lo:hi] = hidden_part(n_ref[...], gu, lo, hi)
    far_ref[...] = down_dot(hid_ref[...], dn, 2)


def third_kernel(hid_ref, dn, rest_ref):
    lhs = hid_ref[...]
    for i, d in enumerate((1, 3, 0)):
        rest_ref[i] = down_dot(lhs, dn, d)


def far_kernel(a_ref, b_ref, right_ref, left_ref):
    h = a_ref.shape[0] // 2
    total = a_ref[...].astype(F32) + b_ref[...].astype(F32)
    right_ref[...] = total[:h].astype(BF)
    left_ref[...] = total[h:].astype(BF)


def near_kernel(a_ref, b_ref, right_ref, left_ref, accr_ref, accl_ref, own_ref):
    h = a_ref.shape[1] // 2
    right_ref[...] = (a_ref[0, h:].astype(F32) + b_ref[0, h:].astype(F32)).astype(BF)
    left_ref[...] = (a_ref[1, :h].astype(F32) + b_ref[1, :h].astype(F32)).astype(BF)
    accr_ref[...] = a_ref[0, :h].astype(F32) + b_ref[0, :h].astype(F32)
    accl_ref[...] = a_ref[1, h:].astype(F32) + b_ref[1, h:].astype(F32)
    own_ref[...] = a_ref[2].astype(F32) + b_ref[2].astype(F32)


def relay_kernel(r_ref, l_ref, accr_ref, accl_ref, right_ref, left_ref):
    right_ref[...] = (r_ref[...].astype(F32) + accr_ref[...]).astype(BF)
    left_ref[...] = (l_ref[...].astype(F32) + accl_ref[...]).astype(BF)


def joined_kernel(own_ref, fl_ref, fr_ref, top_ref, bot_ref, keep_ref, send_ref, sq_ref):
    c = lax.axis_index("c")
    q = top_ref.shape[0]
    for k in range(2 * q // 64):
        lo = 64 * k
        at = slice(lo, lo + 64)
        if lo < q:
            more = fr_ref[at, :].astype(F32) + top_ref[at, :].astype(F32)
        else:
            more = fl_ref[lo - q : lo - q + 64, :].astype(F32) + bot_ref[lo - q : lo - q + 64, :].astype(F32)
        v = (own_ref[at, :] + more).astype(BF)
        for first, core in ((0, 0), (256, 1)):

            @pl.when(c == core)
            def _():
                keep_ref[at, :] = v[:, first : first + 256]

            @pl.when(c != core)
            def _():
                send_ref[at, :] = v[:, first : first + 256]

    for k in range(2 * q // 128):
        t = jnp.zeros((128, 128), F32)
        for ref in (keep_ref, send_ref):
            f = ref[128 * k : 128 * k + 128, :].astype(F32)
            f = f * f
            t = t + f[:, :128] + f[:, 128:]
        row = jnp.sum(t.T, axis=0, keepdims=True)
        for i in range(8):
            sq_ref[i, k : k + 1, :] = row


def final_kernel(keep_ref, got_ref, skeep_ref, sgot_ref, sq_ref, gain_ref, out_ref):
    c = lax.axis_index("c")
    half = keep_ref.shape[0]
    for f_ref, s_ref, core in ((keep_ref, skeep_ref, c), (got_ref, sgot_ref, 1 - c)):
        total = sq_ref[core]
        for i in range(1, 4):
            total = total + sq_ref[2 * i + core]
        scale = lax.rsqrt(total / 2048.0 + EPS)
        for k in range(half // 128):
            at = slice(128 * k, 128 * k + 128)
            col = stretch(scale[k : k + 1, :])
            for j in range(2):
                ln = slice(128 * j, 128 * j + 128)
                v = s_ref[at, ln].astype(F32) + f_ref[at, ln].astype(F32) * col * gain_ref[:, ln]
                out_ref[pl.ds(pl.multiple_of(core * half + 128 * k, 128), 128), ln] = v.astype(BF)


def call(fn, outs, specs, scratch=(), limit=8, out_spec=VM):
    return pl.pallas_call(
        fn,
        out_shape=tuple(jax.ShapeDtypeStruct(s, d) for s, d in outs),
        in_specs=list(specs),
        out_specs=tuple(out_spec for _ in outs),
        scratch_shapes=list(scratch),
        compiler_params=pltpu.CompilerParams(vmem_limit_bytes=limit << 20),
    )


def kept_in_hbm(*arrays):
    return [pltpu.with_memory_space_constraint(a, pltpu.HBM) for a in arrays]


def swapped(block):
    return lax.ppermute(block, "c", cyc(2, 1))


def steps(
    gate_branch, recur_input, doc_ids, conv_taps, gate_map, input_map, decay_level, decay_extra,
    out_weight, residual, mix_gain, pre_gain, ffn_gain, gate_weight, up_weight, down_weight,
):
    rows, width = recur_input.shape
    half = rows // 2
    c = lax.axis_index("c")

    (stacked,) = call(
        pack_kernel,
        [((2112, 128), BF)],
        [HB] * 3,
        [pltpu.VMEM((2112, 128), BF), pltpu.SemaphoreType.DMA((6,))],
        out_spec=HB,
    )(*kept_in_hbm(gate_weight.T, up_weight.T, down_weight))
    (weights,) = kept_in_hbm(lax.all_gather(stacked, SP, axis=0))

    res_keep = lax.dynamic_slice_in_dim(residual, c * half, half, 0)
    res_send = lax.dynamic_slice_in_dim(residual, (1 - c) * half, half, 0)
    rest = jnp.stack([mix_gain, pre_gain])
    levels = []
    for _ in range(3):
        levels.append(lax.reduce_precision(rest, 8, 7))
        rest = rest - levels[-1]
    coded = jnp.stack(levels, axis=1).reshape(6, 256).astype(BF)
    coded = jnp.concatenate([coded, swapped(coded), jnp.zeros((4, 256), BF)])
    res = jnp.concatenate([res_keep, swapped(res_send), coded])
    out_left = lax.ppermute(out_weight, "x", cyc(4, 1))
    res_right = lax.ppermute(res, "x", cyc(4, 3))
    res_left = lax.ppermute(res, "x", cyc(4, 1))
    out_right = lax.ppermute(out_weight, "x", cyc(4, 3))

    tail = jnp.pad(recur_input[rows - 3 :].astype(F32), ((5, 0), (0, 0)))
    tail_ids = jnp.pad(
        jnp.broadcast_to(doc_ids[rows - 3 :].astype(F32)[:, None], (3, width)), ((5, 0), (0, 0))
    )
    rim = lax.ppermute(
        jnp.concatenate([tail, tail_ids]), SP, [(i, i + 1) for i in range(15)]
    )
    nsp = (-8.0 * jax.nn.softplus(-decay_level))[None, :]
    states, products, ends = call(
        scan_kernel,
        [((rows, width), F32), ((rows, width), F32), ((16, 2, width), F32)],
        [VM] * 8,
        [
            pltpu.VMEM((rows + 8, width), F32),
            pltpu.VMEM((rows + 8, width), F32),
            pltpu.VMEM((rows, width), F32),
            pltpu.VMEM((rows, width), F32),
        ],
    )(
        *kept_in_hbm(recur_input),
        rim,
        doc_ids.astype(F32).reshape(rows // 128, 128),
        *kept_in_hbm(conv_taps, gate_map, input_map),
        nsp,
        *kept_in_hbm(decay_extra),
    )
    all_ends = lax.all_to_all(ends, SP, 0, 0, tiled=True)
    (branch,) = call(branch_kernel, [((8, half, width), BF)], [VM] * 4)(
        states, products, all_ends, *kept_in_hbm(gate_branch)
    )
    branch = lax.all_to_all(branch, TP, 0, 0, tiled=True)
    out_far = lax.ppermute(out_left, "x", cyc(4, 1))
    res_far = lax.ppermute(res_right, "x", cyc(4, 3))
    outs = [out_weight, out_left, out_right]
    others = [swapped(b) for b in outs]
    others.append(swapped(out_far))
    outs.append(out_far)
    norm_send, norm_own, skeep, ssend = call(
        mix_kernel,
        [((half, 2048), BF)] * 2 + [((half, 256), BF)] * 2,
        [VM] * 13,
        [
            pltpu.VMEM((half, 1024), BF),
            pltpu.VMEM((half, 2048), BF),
            pltpu.VMEM((half, 2048), BF),
        ],
        limit=12,
    )(branch, *outs, *others, res, res_left, res_right, res_far)
    (norm_own,) = kept_in_hbm(norm_own)
    norm_oth = swapped(norm_send)
    sgot = swapped(ssend)

    far_oth, rest_oth, gate_up, down, norm_own = call(
        first_kernel,
        [
            ((half, 512), BF),
            ((3, half, 512), BF),
            ((16, 1408, 128), BF),
            ((16, 704, 128), BF),
            ((half, 2048), BF),
        ],
        [VM, HB, HB],
        [pltpu.VMEM((half, 704), BF), pltpu.SemaphoreType.DMA((6,))],
        limit=18,
    )(norm_oth, norm_own, weights)
    far_in = swapped(far_oth)
    rest_in = swapped(rest_oth)
    far_own, hid_own = call(
        second_kernel, [((half, 512), BF), ((half, 704), BF)], [VM] * 3, limit=18
    )(norm_own, gate_up, down)
    (rest_own,) = call(third_kernel, [((3, half, 512), BF)], [VM] * 2, limit=14)(hid_own, down)
    q = half // 2
    far_r, far_l = call(far_kernel, [((q, 512), BF)] * 2, [VM] * 2)(far_own, far_in)
    pass_r = lax.ppermute(far_r, "x", cyc(4, 1))
    pass_l = lax.ppermute(far_l, "x", cyc(4, 3))
    near_r, near_l, acc_r, acc_l, own = call(
        near_kernel,
        [((q, 512), BF)] * 2 + [((q, 512), F32)] * 2 + [((half, 512), F32)],
        [VM] * 2,
        limit=10,
    )(rest_own, rest_in)
    from_left = lax.ppermute(near_r, "x", cyc(4, 1))
    from_right = lax.ppermute(near_l, "x", cyc(4, 3))
    pass_r, pass_l = lax.optimization_barrier((pass_r, pass_l))
    right2, left2 = call(relay_kernel, [((q, 512), BF)] * 2, [VM] * 4)(pass_r, pass_l, acc_r, acc_l)
    top = lax.ppermute(right2, "x", cyc(4, 1))
    bottom = lax.ppermute(left2, "x", cyc(4, 3))
    from_left, from_right, top, bottom = lax.optimization_barrier(
        (from_left, from_right, top, bottom)
    )
    fkeep, fsend, square = call(
        joined_kernel,
        [((half, 256), BF)] * 2 + [((8, 3, 128), F32)],
        [VM] * 5,
    )(own, from_left, from_right, top, bottom)
    fgot = swapped(fsend)
    square = lax.all_to_all(square, TP, 0, 0, tiled=True)
    (out,) = call(final_kernel, [((rows, 256), BF)], [VM] * 6)(
        fkeep, fgot, skeep, sgot, square, ffn_gain[None, :]
    )
    return out


def solution(mesh):
    split = Mesh(mesh.devices.reshape(4, 4, 4, 2), ("z", "y", "x", "c"))
    return jax.shard_map(
        steps,
        mesh=split,
        in_specs=(
            P(SP, TP), P(SP, TP), P(SP), P(None, TP), P(TP, None, None), P(TP, None, None), P(TP),
            P(SP, TP), P(None, TP), P(SP, TP), P(TP), P(TP), P(TP), P(SP, TP), P(SP, TP), P(TP, SP),
        ),
        out_specs=P(SP, TP),
        check_vma=False,
    )
```

```python
import jax
import jax.numpy as jnp
from jax import lax
from jax.experimental import pallas as pl
from jax.experimental.pallas import tpu as pltpu
from jax.sharding import Mesh
from jax.sharding import PartitionSpec as P

SP = ("z", "y")
TP = ("x", "c")
EPS = 1e-06
BF = jnp.bfloat16
F32 = jnp.float32
VM = pl.BlockSpec(memory_space=pltpu.VMEM)
HB = pl.BlockSpec(memory_space=pltpu.HBM)
SEGS = 8


def cyc(count, step):
    return [(i, (i + step) % count) for i in range(count)]


def stretch(row, lanes=128):
    return jnp.broadcast_to(row, (lanes, 128)).T


def taylor_expm1_neg(y):
    p = 1.0 + y * (1.0 / 8.0)
    for k in (7.0, 6.0, 5.0, 4.0, 3.0, 2.0):
        p = 1.0 + y * (1.0 / k) * p
    return -y * p


def pack_kernel(g_ref, u_ref, d_ref, out_ref, buf, sem):
    spans = [pl.ds(704 * i, 704) for i in range(3)]
    fetches = [
        pltpu.make_async_copy(ref, buf.at[span], sem.at[i])
        for i, (ref, span) in enumerate(zip((g_ref, u_ref, d_ref), spans))
    ]
    stores = [
        pltpu.make_async_copy(buf.at[span], out_ref.at[span], sem.at[3 + i])
        for i, span in enumerate(spans)
    ]
    for cp in fetches:
        cp.start()
    for cp, then in zip(fetches, stores):
        cp.wait()
        then.start()
    for cp in stores:
        cp.wait()


def scan_kernel(
    x_ref, rim_ref, ids_ref, taps_ref, gm_ref, im_ref, nsp_ref, extra_ref,
    s_ref, p_ref, e_ref, xs, idx, fs, ds,
):
    rows = x_ref.shape[0]
    taps = taps_ref[...].astype(F32)
    head = gm_ref.shape[1]

    def blockdiag(ref):
        zero = jnp.zeros((head, head), BF)
        return jnp.concatenate(
            [
                jnp.concatenate([ref[0], zero], axis=1),
                jnp.concatenate([zero, ref[1]], axis=1),
            ],
            axis=0,
        )

    gate = blockdiag(gm_ref)
    inp = blockdiag(im_ref)
    xs[0:8, :] = rim_ref[0:8, :]
    idx[0:8, :] = rim_ref[8:16, :]
    for j in range(rows // 128):
        at = 8 + 128 * j
        xs[at : at + 128, :] = x_ref[128 * j : 128 * j + 128, :].astype(F32)
        idx[at : at + 128, :] = stretch(ids_ref[j : j + 1, :])
    for j in range(rows // 128):
        at = 8 + 128 * j
        here = idx[at : at + 128, :]
        before = idx[at - 1 : at + 127, :]
        conv = xs[at : at + 128, :] * taps[0:1, :]
        for k in range(1, 4):
            old = idx[at - k : at - k + 128, :]
            conv = conv + jnp.where(old == here, xs[at - k : at - k + 128, :], 0.0) * taps[k : k + 1, :]
        conv = conv.astype(BF)
        rg = jax.nn.sigmoid(jnp.dot(conv, gate, preferred_element_type=F32))
        ig = jax.nn.sigmoid(jnp.dot(conv, inp, preferred_element_type=F32))
        ld = nsp_ref[...] * rg + extra_ref[128 * j : 128 * j + 128, :]
        e = jnp.exp(ld)
        y = 2.0 * ld
        em = jnp.where(y > -0.5, taylor_expm1_neg(jnp.maximum(y, -0.5)), 1.0 - e * e)
        fs[128 * j : 128 * j + 128, :] = jnp.where(before == here, e, 0.0)
        ds[128 * j : 128 * j + 128, :] = jnp.sqrt(em) * ig * conv.astype(F32)
    seg = rows // SEGS

    def step(j, carry):
        h, p = carry
        f = fs[pl.ds(j, SEGS, stride=seg), :]
        d = ds[pl.ds(j, SEGS, stride=seg), :]
        h = f * h + d
        p = p * f
        s_ref[pl.ds(j, SEGS, stride=seg), :] = h
        p_ref[pl.ds(j, SEGS, stride=seg), :] = p
        return h, p

    zero = jnp.zeros((SEGS, 128), F32)
    h, p = lax.fori_loop(0, seg, step, (zero, zero + 1.0), unroll=8)
    a = p[0:1, :]
    b = h[0:1, :]
    for s in range(1, SEGS):
        b = p[s : s + 1, :] * b + h[s : s + 1, :]
        a = p[s : s + 1, :] * a
    for i in range(16):
        e_ref[i, 0:1, :] = a
        e_ref[i, 1:2, :] = b


def branch_kernel(s_ref, p_ref, e_ref, g_ref, out_ref):
    rows = s_ref.shape[0]
    seg = rows // SEGS
    me = lax.axis_index(SP)
    h = jnp.zeros((1, 128), F32)
    for i in range(16):
        a = e_ref[i, 0:1, :]
        b = e_ref[i, 1:2, :]
        h = jnp.where(i < me, a * h + b, h)
    half = SEGS // 2
    for s in range(SEGS):
        at = s * seg
        st = s_ref[at : at + seg, :]
        pr = p_ref[at : at + seg, :]
        states = st + pr * h
        out = (states * jax.nn.gelu(g_ref[at : at + seg, :].astype(F32), approximate=True)).astype(BF)
        h = states[seg - 1 : seg, :]
        to = (s % half) * seg
        for i in range(4):
            out_ref[2 * i + s // half, to : to + seg, :] = out


def mix_kernel(
    br_ref, w0, w1, w2, w3, v0, v1, v2, v3, r0, r1, r2, r3,
    norm_ref, also_ref, keep_ref, send_ref, full, mixed, stream,
):
    x = lax.axis_index("x")
    c = lax.axis_index("c")
    rows = br_ref.shape[1]
    for i in range(8):
        full[:, 128 * i : 128 * i + 128] = br_ref[i]
    lhs = full[...]
    total = jnp.zeros((rows, 128), F32)
    pieces = []
    for d, w, v, r in ((0, w0, v0, r0), (3, w1, v1, r1), (1, w2, v2, r2), (2, w3, v3, r3)):
        block = lax.rem(x + d, 4)
        g = r[2 * rows : 2 * rows + 16, :].astype(F32)
        for k, core, ref in ((0, c, w), (1, 1 - c, v)):
            at = pl.ds(pl.multiple_of((2 * block + core) * 256, 256), 256)
            m = 6 * k
            pieces.append(
                (
                    at,
                    r,
                    rows * k,
                    g[m : m + 1] + g[m + 1 : m + 2] + g[m + 2 : m + 3],
                    g[m + 3 : m + 4] + g[m + 4 : m + 5] + g[m + 5 : m + 6],
                )
            )
            m = jnp.dot(lhs, ref[...], preferred_element_type=F32).astype(BF)
            mixed[:, at] = m
            mf = m.astype(F32)
            mf = mf * mf
            total = total + mf[:, :128] + mf[:, 128:]
    scale = lax.rsqrt(jnp.sum(total, axis=1, keepdims=True) / 2048.0 + EPS)
    total = jnp.zeros((rows, 128), F32)
    for at, res, lo, mg, _ in pieces:
        r = res[lo : lo + rows, :].astype(F32)
        s = (r + mixed[:, at].astype(F32) * scale * mg).astype(BF)
        stream[:, at] = s
        sf = s.astype(F32)
        sf = sf * sf
        total = total + sf[:, :128] + sf[:, 128:]
    scale = lax.rsqrt(jnp.sum(total, axis=1, keepdims=True) / 2048.0 + EPS)
    for at, _, _, _, pg in pieces:
        n = (stream[:, at].astype(F32) * scale * pg).astype(BF)
        norm_ref[:, at] = n
        also_ref[:, at] = n
    keep_ref[...] = stream[:, pl.ds(pl.multiple_of((2 * x + c) * 256, 256), 256)]
    send_ref[...] = stream[:, pl.ds(pl.multiple_of((2 * x + 1 - c) * 256, 256), 256)]


def down_dot(lhs, dn, d):
    first = 4 * lax.rem(lax.axis_index("x") + d, 4)
    part = jnp.concatenate([dn[first + i] for i in range(4)], axis=1)
    return jnp.dot(lhs, part, preferred_element_type=F32).astype(BF)


CUTS = ((0, 128), (128, 384), (384, 640), (640, 704))


def hidden_part(src, gu, lo, hi):
    rows = [
        jnp.concatenate([gu[s, base + lo : base + hi, :] for s in range(16)], axis=1)
        for base in (0, 704)
    ]
    act = lax.dot_general(
        src, jnp.concatenate(rows), (((1,), (1,)), ((), ())), preferred_element_type=F32
    )
    return (jax.nn.silu(act[:, : hi - lo]) * act[:, hi - lo :]).astype(BF)


def first_kernel(n_ref, own_hbm, w_ref, far_ref, rest_ref, gu, dn, own_ref, hid, sem):
    groups = []
    for i, (lo, hi) in enumerate(CUTS):
        groups.append(
            [
                pltpu.make_async_copy(
                    w_ref.at[s, pl.ds(base + lo, hi - lo)],
                    gu.at[s, pl.ds(base + lo, hi - lo)],
                    sem.at[i],
                )
                for s in range(16)
                for base in (0, 704)
            ]
        )
    downs = [
        pltpu.make_async_copy(w_ref.at[s, pl.ds(1408, 704)], dn.at[s], sem.at[4]) for s in range(16)
    ]
    own_copy = pltpu.make_async_copy(own_hbm, own_ref, sem.at[5])
    for group in groups + [downs, [own_copy]]:
        for cp in group:
            cp.start()
    for (lo, hi), group in zip(CUTS, groups):
        for cp in group:
            cp.wait()
        hid[:, lo:hi] = hidden_part(n_ref[...], gu, lo, hi)
    for cp in downs:
        cp.wait()
    lhs = hid[...]
    far_ref[...] = down_dot(lhs, dn, 2)
    for i, d in enumerate((1, 3, 0)):
        rest_ref[i] = down_dot(lhs, dn, d)
    own_copy.wait()


def second_kernel(n_ref, gu, dn, far_ref, hid_ref):
    for lo, hi in CUTS:
        hid_ref[:, lo:hi] = hidden_part(n_ref[...], gu, lo, hi)
    far_ref[...] = down_dot(hid_ref[...], dn, 2)


def third_kernel(hid_ref, dn, rest_ref):
    lhs = hid_ref[...]
    for i, d in enumerate((1, 3, 0)):
        rest_ref[i] = down_dot(lhs, dn, d)


def far_kernel(a_ref, b_ref, right_ref, left_ref):
    h = a_ref.shape[0] // 2
    total = a_ref[...].astype(F32) + b_ref[...].astype(F32)
    right_ref[...] = total[:h].astype(BF)
    left_ref[...] = total[h:].astype(BF)


def near_kernel(a_ref, b_ref, right_ref, left_ref, accr_ref, accl_ref, own_ref):
    h = a_ref.shape[1] // 2
    right_ref[...] = (a_ref[0, h:].astype(F32) + b_ref[0, h:].astype(F32)).astype(BF)
    left_ref[...] = (a_ref[1, :h].astype(F32) + b_ref[1, :h].astype(F32)).astype(BF)
    accr_ref[...] = a_ref[0, :h].astype(F32) + b_ref[0, :h].astype(F32)
    accl_ref[...] = a_ref[1, h:].astype(F32) + b_ref[1, h:].astype(F32)
    own_ref[...] = a_ref[2].astype(F32) + b_ref[2].astype(F32)


def relay_kernel(r_ref, l_ref, accr_ref, accl_ref, right_ref, left_ref):
    right_ref[...] = (r_ref[...].astype(F32) + accr_ref[...]).astype(BF)
    left_ref[...] = (l_ref[...].astype(F32) + accl_ref[...]).astype(BF)


def joined_kernel(own_ref, fl_ref, fr_ref, top_ref, bot_ref, keep_ref, send_ref, sq_ref):
    c = lax.axis_index("c")
    q = top_ref.shape[0]
    for k in range(2 * q // 64):
        lo = 64 * k
        at = slice(lo, lo + 64)
        if lo < q:
            more = fr_ref[at, :].astype(F32) + top_ref[at, :].astype(F32)
        else:
            more = fl_ref[lo - q : lo - q + 64, :].astype(F32) + bot_ref[lo - q : lo - q + 64, :].astype(F32)
        v = (own_ref[at, :] + more).astype(BF)
        low, high = v[:, :256], v[:, 256:]
        keep_ref[at, :] = jnp.where(c == 0, low, high)
        send_ref[at, :] = jnp.where(c == 0, high, low)

    for k in range(2 * q // 128):
        t = jnp.zeros((128, 128), F32)
        for ref in (keep_ref, send_ref):
            f = ref[128 * k : 128 * k + 128, :].astype(F32)
            f = f * f
            t = t + f[:, :128] + f[:, 128:]
        row = jnp.sum(t.T, axis=0, keepdims=True)
        for i in range(8):
            sq_ref[i, k : k + 1, :] = row


def final_kernel(keep_ref, got_ref, skeep_ref, sgot_ref, sq_ref, gain_ref, out_ref):
    c = lax.axis_index("c")
    half = keep_ref.shape[0]
    for f_ref, s_ref, core in ((keep_ref, skeep_ref, c), (got_ref, sgot_ref, 1 - c)):
        total = sq_ref[core]
        for i in range(1, 4):
            total = total + sq_ref[2 * i + core]
        scale = lax.rsqrt(total / 2048.0 + EPS)
        for k in range(half // 128):
            at = slice(128 * k, 128 * k + 128)
            col = stretch(scale[k : k + 1, :])
            for j in range(2):
                ln = slice(128 * j, 128 * j + 128)
                v = s_ref[at, ln].astype(F32) + f_ref[at, ln].astype(F32) * col * gain_ref[:, ln]
                out_ref[pl.ds(pl.multiple_of(core * half + 128 * k, 128), 128), ln] = v.astype(BF)


def call(fn, outs, specs, scratch=(), limit=8, out_spec=VM):
    return pl.pallas_call(
        fn,
        out_shape=tuple(jax.ShapeDtypeStruct(s, d) for s, d in outs),
        in_specs=list(specs),
        out_specs=tuple(out_spec for _ in outs),
        scratch_shapes=list(scratch),
        compiler_params=pltpu.CompilerParams(vmem_limit_bytes=limit << 20),
    )


def kept_in_hbm(*arrays):
    return [pltpu.with_memory_space_constraint(a, pltpu.HBM) for a in arrays]


def swapped(block):
    return lax.ppermute(block, "c", cyc(2, 1))


def steps(
    gate_branch, recur_input, doc_ids, conv_taps, gate_map, input_map, decay_level, decay_extra,
    out_weight, residual, mix_gain, pre_gain, ffn_gain, gate_weight, up_weight, down_weight,
):
    rows, width = recur_input.shape
    half = rows // 2
    c = lax.axis_index("c")

    (stacked,) = call(
        pack_kernel,
        [((2112, 128), BF)],
        [HB] * 3,
        [pltpu.VMEM((2112, 128), BF), pltpu.SemaphoreType.DMA((6,))],
        out_spec=HB,
    )(*kept_in_hbm(gate_weight.T, up_weight.T, down_weight))
    (weights,) = kept_in_hbm(lax.all_gather(stacked, SP, axis=0))

    res_keep = lax.dynamic_slice_in_dim(residual, c * half, half, 0)
    res_send = lax.dynamic_slice_in_dim(residual, (1 - c) * half, half, 0)
    rest = jnp.stack([mix_gain, pre_gain])
    levels = []
    for _ in range(3):
        levels.append(lax.reduce_precision(rest, 8, 7))
        rest = rest - levels[-1]
    coded = jnp.stack(levels, axis=1).reshape(6, 256).astype(BF)
    coded = jnp.concatenate([coded, swapped(coded), jnp.zeros((4, 256), BF)])
    res = jnp.concatenate([res_keep, swapped(res_send), coded])
    out_left = lax.ppermute(out_weight, "x", cyc(4, 1))
    res_right = lax.ppermute(res, "x", cyc(4, 3))
    res_left = lax.ppermute(res, "x", cyc(4, 1))
    out_right = lax.ppermute(out_weight, "x", cyc(4, 3))

    tail = jnp.pad(recur_input[rows - 3 :].astype(F32), ((5, 0), (0, 0)))
    tail_ids = jnp.pad(
        jnp.broadcast_to(doc_ids[rows - 3 :].astype(F32)[:, None], (3, width)), ((5, 0), (0, 0))
    )
    rim = lax.ppermute(
        jnp.concatenate([tail, tail_ids]), SP, [(i, i + 1) for i in range(15)]
    )
    nsp = (-8.0 * jax.nn.softplus(-decay_level))[None, :]
    states, products, ends = call(
        scan_kernel,
        [((rows, width), F32), ((rows, width), F32), ((16, 2, width), F32)],
        [VM] * 8,
        [
            pltpu.VMEM((rows + 8, width), F32),
            pltpu.VMEM((rows + 8, width), F32),
            pltpu.VMEM((rows, width), F32),
            pltpu.VMEM((rows, width), F32),
        ],
    )(
        *kept_in_hbm(recur_input),
        rim,
        doc_ids.astype(F32).reshape(rows // 128, 128),
        *kept_in_hbm(conv_taps, gate_map, input_map),
        nsp,
        *kept_in_hbm(decay_extra),
    )
    all_ends = lax.all_to_all(ends, SP, 0, 0, tiled=True)
    (branch,) = call(branch_kernel, [((8, half, width), BF)], [VM] * 4)(
        states, products, all_ends, *kept_in_hbm(gate_branch)
    )
    branch = lax.all_to_all(branch, TP, 0, 0, tiled=True)
    out_far = lax.ppermute(out_left, "x", cyc(4, 1))
    res_far = lax.ppermute(res_right, "x", cyc(4, 3))
    outs = [out_weight, out_left, out_right]
    others = [swapped(b) for b in outs]
    others.append(swapped(out_far))
    outs.append(out_far)
    norm_send, norm_own, skeep, ssend = call(
        mix_kernel,
        [((half, 2048), BF)] * 2 + [((half, 256), BF)] * 2,
        [VM] * 13,
        [
            pltpu.VMEM((half, 1024), BF),
            pltpu.VMEM((half, 2048), BF),
            pltpu.VMEM((half, 2048), BF),
        ],
        limit=12,
    )(branch, *outs, *others, res, res_left, res_right, res_far)
    (norm_own,) = kept_in_hbm(norm_own)
    norm_oth = swapped(norm_send)
    sgot = swapped(ssend)

    far_oth, rest_oth, gate_up, down, norm_own = call(
        first_kernel,
        [
            ((half, 512), BF),
            ((3, half, 512), BF),
            ((16, 1408, 128), BF),
            ((16, 704, 128), BF),
            ((half, 2048), BF),
        ],
        [VM, HB, HB],
        [pltpu.VMEM((half, 704), BF), pltpu.SemaphoreType.DMA((6,))],
        limit=18,
    )(norm_oth, norm_own, weights)
    far_in = swapped(far_oth)
    rest_in = swapped(rest_oth)
    far_own, hid_own = call(
        second_kernel, [((half, 512), BF), ((half, 704), BF)], [VM] * 3, limit=18
    )(norm_own, gate_up, down)
    (rest_own,) = call(third_kernel, [((3, half, 512), BF)], [VM] * 2, limit=14)(hid_own, down)
    q = half // 2
    far_r, far_l = call(far_kernel, [((q, 512), BF)] * 2, [VM] * 2)(far_own, far_in)
    pass_r = lax.ppermute(far_r, "x", cyc(4, 1))
    pass_l = lax.ppermute(far_l, "x", cyc(4, 3))
    near_r, near_l, acc_r, acc_l, own = call(
        near_kernel,
        [((q, 512), BF)] * 2 + [((q, 512), F32)] * 2 + [((half, 512), F32)],
        [VM] * 2,
        limit=10,
    )(rest_own, rest_in)
    from_left = lax.ppermute(near_r, "x", cyc(4, 1))
    from_right = lax.ppermute(near_l, "x", cyc(4, 3))
    pass_r, pass_l = lax.optimization_barrier((pass_r, pass_l))
    right2, left2 = call(relay_kernel, [((q, 512), BF)] * 2, [VM] * 4)(pass_r, pass_l, acc_r, acc_l)
    top = lax.ppermute(right2, "x", cyc(4, 1))
    bottom = lax.ppermute(left2, "x", cyc(4, 3))
    from_left, from_right, top, bottom = lax.optimization_barrier(
        (from_left, from_right, top, bottom)
    )
    fkeep, fsend, square = call(
        joined_kernel,
        [((half, 256), BF)] * 2 + [((8, 3, 128), F32)],
        [VM] * 5,
    )(own, from_left, from_right, top, bottom)
    fgot = swapped(fsend)
    square = lax.all_to_all(square, TP, 0, 0, tiled=True)
    (out,) = call(final_kernel, [((rows, 256), BF)], [VM] * 6)(
        fkeep, fgot, skeep, sgot, square, ffn_gain[None, :]
    )
    return out


def solution(mesh):
    split = Mesh(mesh.devices.reshape(4, 4, 4, 2), ("z", "y", "x", "c"))
    return jax.shard_map(
        steps,
        mesh=split,
        in_specs=(
            P(SP, TP), P(SP, TP), P(SP), P(None, TP), P(TP, None, None), P(TP, None, None), P(TP),
            P(SP, TP), P(None, TP), P(SP, TP), P(TP), P(TP), P(TP), P(SP, TP), P(SP, TP), P(TP, SP),
        ),
        out_specs=P(SP, TP),
        check_vma=False,
    )
```
